512 devices in a mesh: sp: 64 (over z, y), dp: 8 (over x, core).
Axes of the slice: x: 4, y: 4, z: 16, core: 2. Of those that a mesh axis runs over, the one named last changes fastest.
Arguments:
- tokens: bfloat16 [8, 8192, 2048], P('dp', 'sp'), may hold values from -6 to 6
- w_value: bfloat16 [2048, 1024], P('dp', 'sp'), may hold values from -0.125 to 0.125
- w_gate: bfloat16 [2048, 1024], P('dp', 'sp'), may hold values from -0.125 to 0.125
- w_out: bfloat16 [1024, 2048], P('dp', 'sp'), may hold values from -0.1875 to 0.1875
- conv_taps: bfloat16 [1024, 31], replicated, may hold values from -1 to 1
- norm_gain: float32 [1024], replicated, may hold values from 0.1 to 1.9
- norm_bias: float32 [1024], replicated, may hold values from -3 to 3
Outputs:
- mixed: bfloat16 [8, 8192, 2048], P('dp', 'sp')
The draws below stay inside these ranges and needn't reach their ends.
All inputs are finite; a program needn't handle non-finite values.
Results may differ from the reference program's by a relative error of at most 0.0064.
Values may be sent and summed in bfloat16 or wider, within the bound.
A program may use at most 64 MiB of HBM per device.

```python
import jax
import jax.numpy as jnp
from jax import lax

D = 2048
CH = 1024
KW = 31
SEQ = 8192
SEQS = 8


def levels(stream_key, shape, shards, smallest, largest):
    gain = 1.0
    for position, blocks in shards:
        heights = jax.random.uniform(jax.random.fold_in(jax.random.fold_in(stream_key, 6), position), (blocks,), jnp.float32, smallest / len(shards), largest / len(shards))
        gain = gain * jnp.repeat(jnp.exp(heights), shape[position] // blocks).reshape((-1,) + (1,) * (len(shape) - 1 - position))
    return gain


def scatter_about(stream_key, dims, deviation, limit, split=(), held_as=jnp.bfloat16):
    entries = deviation * jax.random.normal(stream_key, dims, jnp.float32)
    if split:
        entries = entries * levels(stream_key, dims, split, -0.22, 0.18)
    return jnp.clip(entries, -limit, limit).astype(held_as)


def setup_inputs(seed: int = 0) -> dict:
    key_list = jax.random.split(jax.random.key(seed), 8)
    tokens = scatter_about(key_list[0], (SEQS, SEQ, D), 1.0, 6.0, ((0, 8), (1, 64)))
    w_value = scatter_about(key_list[1], (D, CH), D ** -0.5, 0.125, ((0, 8), (1, 64)))
    w_gate = scatter_about(key_list[2], (D, CH), D ** -0.5, 0.125, ((0, 8), (1, 64)))
    w_out = scatter_about(key_list[3], (CH, D), CH ** -0.5, 0.1875, ((0, 8), (1, 64)))
    conv_taps = scatter_about(key_list[4], (CH, KW), KW ** -0.5, 1.0)
    norm_gain = jnp.clip(1.0 + 0.18 * jax.random.normal(key_list[5], (CH,), jnp.float32), 0.1, 1.9)
    norm_bias = scatter_about(key_list[6], (CH,), 0.5, 3.0, (), jnp.float32)
    return {"tokens": tokens, "w_value": w_value, "w_gate": w_gate, "w_out": w_out, "conv_taps": conv_taps, "norm_gain": norm_gain, "norm_bias": norm_bias}


def reference(tokens, w_value, w_gate, w_out, conv_taps, norm_gain, norm_bias):
    margin = KW // 2
    taps = conv_taps.astype(jnp.float32).T

    def one_sequence(seq_rows):
        value = jnp.dot(seq_rows, w_value, preferred_element_type=jnp.float32)
        gate = jnp.dot(seq_rows, w_gate, preferred_element_type=jnp.float32)
        gated = lax.optimization_barrier((value * jax.nn.sigmoid(gate)).astype(jnp.bfloat16))
        padded = jnp.pad(gated, ((margin, margin), (0, 0))).astype(jnp.float32)
        total = jnp.zeros((SEQ, CH), jnp.float32)
        for offset in range(KW):
            total = total + padded[offset:offset + SEQ] * taps[offset][None, :]
        conv = lax.optimization_barrier(total.astype(jnp.bfloat16)).astype(jnp.float32)
        mean = lax.optimization_barrier(jnp.mean(conv, axis=-1, keepdims=True))
        centred = conv - mean
        variance = lax.optimization_barrier(jnp.mean(centred * centred, axis=-1, keepdims=True))
        normed = centred * lax.rsqrt(variance + 1e-05) * norm_gain[None, :] + norm_bias[None, :]
        act = (normed * jax.nn.sigmoid(normed)).astype(jnp.bfloat16)
        return jnp.dot(act, w_out, preferred_element_type=jnp.float32).astype(jnp.bfloat16)
    return lax.map(one_sequence, tokens)
```

```python
import jax
import jax.numpy as jnp
from jax import lax
from jax.experimental import pallas as pl
from jax.experimental.pallas import tpu as pltpu
from jax.sharding import PartitionSpec as P

MESH = pl.DeviceIdType.MESH
NSEM = 240
NT = (((1,), (1,)), ((), ()))


def kernel(tok, wv, wg, wo, taps, gain, bias, out, W, O, X, T, CV, ACT, ssem, rsem, lsem):
    sp = lax.axis_index("sp")
    dp = lax.axis_index("dp")
    z, y = sp // 4, lax.rem(sp, 4)
    x, c = dp // 2, lax.rem(dp, 2)
    q, r = z // 4, lax.rem(z, 4)

    def dev(x=x, y=y, z=z, c=c):
        return {"sp": z * 4 + y, "dp": x * 2 + c}

    def mod(v, n):
        return lax.rem(v + n, n)

    xl, xr = mod(x - 1, 4), mod(x + 1, 4)
    yl, yr = mod(y - 1, 4), mod(y + 1, 4)
    zl, zr = mod(z - 1, 16), mod(z + 1, 16)
    z4l, z4r = mod(z - 4, 16), mod(z + 4, 16)
    peers = [q * 4 + mod(r + d, 4) for d in (1, 2, 3)]
    qs = [q, mod(q - 1, 4), mod(q + 1, 4), mod(q + 2, 4)]
    prev, nxt = mod(sp - 1, 64), mod(sp + 1, 64)

    local = [
        pltpu.make_async_copy(wv, W.at[x, c, q, r, y, 0], lsem.at[0]),
        pltpu.make_async_copy(wg, W.at[x, c, q, r, y, 1], lsem.at[1]),
        pltpu.make_async_copy(wo, O.at[x, c, z, y], lsem.at[2]),
        pltpu.make_async_copy(tok, X.at[pl.ds(16, 128)], lsem.at[3]),
    ]
    for d in local:
        d.start()

    barrier = pltpu.get_barrier_semaphore()
    partners = [dev(x=xl), dev(x=xr), dev(y=yl), dev(y=yr), dev(z=zl), dev(z=zr), dev(z=z4l), dev(z=z4r)]
    partners += [dev(z=p) for p in peers]
    partners += [dev(c=1 - c), {"sp": prev, "dp": dp}, {"sp": nxt, "dp": dp}]
    for p in partners:
        pl.semaphore_signal(barrier, inc=1, device_id=p, device_id_type=MESH)

    T[...] = taps[...].astype(jnp.float32)

    @pl.when(sp == 0)
    def _():
        X[pl.ds(0, 16), :] = jnp.zeros((16, 2048), jnp.bfloat16)

    @pl.when(sp == 63)
    def _():
        X[pl.ds(144, 16), :] = jnp.zeros((16, 2048), jnp.bfloat16)

    pl.semaphore_wait(barrier, len(partners))
    for d in local:
        d.wait()

    sends = []
    count = [0]

    def describe(src, dst, to):
        i = count[0]
        count[0] += 1
        return pltpu.make_async_remote_copy(
            src_ref=src, dst_ref=dst, send_sem=ssem.at[i], recv_sem=rsem.at[i],
            device_id=to, device_id_type=MESH,
        )

    def send(ref, to):
        d = describe(ref, ref, to)
        d.start()
        sends.append(d)
        return d

    events = []
    st = {}

    def at(t):
        def add(f):
            events.append((t, len(events), f))
        return add

    halo_r = describe(X.at[pl.ds(128, 16)], X.at[pl.ds(0, 16)], {"sp": nxt, "dp": dp})
    halo_l = describe(X.at[pl.ds(16, 16)], X.at[pl.ds(144, 16)], {"sp": prev, "dp": dp})

    @at(0.9)
    def _():
        @pl.when(sp < 63)
        def _():
            halo_r.start()

        @pl.when(sp > 0)
        def _():
            halo_l.start()

    @at(0.1)
    def _():
        b = O.at[x, c, z, y]
        st["ox"] = (send(b, dev(x=xr)), send(b, dev(x=xl)))

    @at(2.4)
    def _():
        a, b = st["ox"]
        a.wait_recv()
        e = send(O.at[xl, c, z, y, pl.ds(0, 16)], dev(x=xr))
        b.wait_recv()
        st["ox2"] = (e, send(O.at[xr, c, z, y, pl.ds(16, 16)], dev(x=xl)))

    @at(4.7)
    def _():
        for d in st["ox2"]:
            d.wait_recv()
        b = O.at[:, c, z, y]
        st["oy"] = (send(b, dev(y=yr)), send(b, dev(y=yl)))

    @at(7.2)
    def _():
        a, b = st["oy"]
        a.wait_recv()
        e = send(O.at[pl.ds(0, 2), c, z, yl], dev(y=yr))
        b.wait_recv()
        st["oy2"] = (e, send(O.at[pl.ds(2, 2), c, z, yr], dev(y=yl)))

    def ring_sends(s):
        zo, zp = mod(z - s, 16), mod(z + s, 16)
        for h in (0, 1):
            if s < 8:
                st["r", s, h] = send(O.at[:, c, zo, pl.ds(2 * h, 2)], dev(z=zr))
            if s < 7:
                st["l", s, h] = send(O.at[:, c, zp, pl.ds(2 * h, 2)], dev(z=zl))

    @at(9.6)
    def _():
        for d in st["oy2"]:
            d.wait_recv()
        ring_sends(0)
        st["od", 0] = [send(O.at[:, c, z], dev(c=1 - c))]

    def ring(s):
        zo, zp = mod(z - s, 16), mod(z + s, 16)
        for h in (0, 1):
            st["r", s - 1, h].wait_recv()
            if s < 8:
                st["r", s, h] = send(O.at[:, c, zo, pl.ds(2 * h, 2)], dev(z=zr))
            if s < 8:
                st["l", s - 1, h].wait_recv()
            if s < 7:
                st["l", s, h] = send(O.at[:, c, zp, pl.ds(2 * h, 2)], dev(z=zl))
        st["od", s] = [send(O.at[:, c, zo], dev(c=1 - c))]
        if s < 8:
            st["od", s].append(send(O.at[:, c, zp], dev(c=1 - c)))

    for s in range(1, 9):
        at(10 + 3.3 * s)(lambda s=s: ring(s))

    @at(0.0)
    def _():
        b = W.at[x, c, q, r, y]
        st["s2", 0] = [send(b, dev(z=p)) for p in peers]
        st["s1"] = (send(b, dev(z=z4r)), send(b, dev(z=z4l)))

    @at(4.2)
    def _():
        a, b = st["s1"]
        a.wait_recv()
        e = send(W.at[x, c, qs[1], r, y, 0], dev(z=z4r))
        b.wait_recv()
        st["s1b"] = (e, send(W.at[x, c, qs[2], r, y, 1], dev(z=z4l)))
        for m in (1, 2):
            st["s2", m] = [send(W.at[x, c, qs[m], r, y], dev(z=p)) for p in peers]

    @at(8.2)
    def _():
        for d in st["s1b"]:
            d.wait_recv()
        st["s2", 3] = [send(W.at[x, c, qs[3], r, y], dev(z=p)) for p in peers]

    def p1(m):
        for d in st["s2", m]:
            d.wait_recv()
        A, B = W.at[x, c, qs[m], :, y, 0], W.at[x, c, qs[m], :, y, 1]
        st["p1", m] = (send(A, dev(y=yr)), send(A, dev(y=yl)), send(B, dev(x=xr)), send(B, dev(x=xl)))

    def p1r(m):
        a, b, e, f = st["p1", m]
        lo, hi = pl.ds(0, 2), pl.ds(2, 2)
        a.wait_recv()
        g = [send(W.at[x, c, qs[m], lo, yl, 0], dev(y=yr))]
        b.wait_recv()
        g.append(send(W.at[x, c, qs[m], hi, yr, 0], dev(y=yl)))
        e.wait_recv()
        g.append(send(W.at[xl, c, qs[m], lo, y, 1], dev(x=xr)))
        f.wait_recv()
        g.append(send(W.at[xr, c, qs[m], hi, y, 1], dev(x=xl)))
        st["p1r", m] = g

    def p2(m):
        for d in st["p1r", m]:
            d.wait_recv()
        A, B = W.at[x, c, qs[m], :, :, 0], W.at[:, c, qs[m], :, y, 1]
        st["p2", m] = (send(A, dev(x=xr)), send(A, dev(x=xl)), send(B, dev(y=yr)), send(B, dev(y=yl)))

    def p2r(m):
        a, b, e, f = st["p2", m]
        lo, hi = pl.ds(0, 2), pl.ds(2, 2)
        a.wait_recv()
        g = [send(W.at[xl, c, qs[m], lo, :, 0], dev(x=xr))]
        b.wait_recv()
        g.append(send(W.at[xr, c, qs[m], hi, :, 0], dev(x=xl)))
        e.wait_recv()
        g.append(send(W.at[:, c, qs[m], lo, yl, 1], dev(y=yr)))
        f.wait_recv()
        g.append(send(W.at[:, c, qs[m], hi, yr, 1], dev(y=yl)))
        st["p2r", m] = g

    def d2d(m):
        for d in st["p2r", m]:
            d.wait_recv()
        st["d2d", m] = [send(W.at[:, c, qs[m], :, :, k], dev(c=1 - c)) for k in (0, 1)]

    def compute(m):
        for d in st["d2d", m]:
            d.wait_recv()
        if m == 0:
            @pl.when(sp > 0)
            def _():
                halo_r.wait_recv()

            @pl.when(sp < 63)
            def _():
                halo_l.wait_recv()

        qm = qs[m]
        acc = [None, None]
        for i in range(8):
            xs = X[:, 256 * i : 256 * i + 256]
            for k in (0, 1):
                w = W[i // 2, i % 2, qm, :, :, k].reshape(256, 256)
                part = lax.dot_general(xs, w, NT, preferred_element_type=jnp.float32)
                acc[k] = part if acc[k] is None else acc[k] + part
        gated = (acc[0] * jax.nn.sigmoid(acc[1])).astype(jnp.bfloat16).astype(jnp.float32)
        for h in (0, 1):
            strip = gated[:, 128 * h : 128 * h + 128]
            lanes = pl.ds(pl.multiple_of(qm * 256 + 128 * h, 128), 128)
            total = jnp.zeros((128, 128), jnp.float32)
            for shift in range(8):
                rolled = strip if shift == 0 else pltpu.roll(strip, 160 - shift, 0)
                for k in range(31):
                    if (k + 1) % 8 == shift:
                        first = (k + 1) // 8 * 8
                        total = total + T[pl.ds(k, 1), lanes] * rolled[first : first + 128]
            CV[:, lanes] = total.astype(jnp.bfloat16).astype(jnp.float32)

    t1 = [3.4, 7.6, 7.7, 11.4]
    t2 = [8.1, 12.6, 13.2, 16.4]
    t3 = [13.5, 17.8, 22.0, 26.2]
    for m in range(4):
        at(t1[m])(lambda m=m: p1(m))
        at(t1[m] + 2.3)(lambda m=m: p1r(m))
        at(t2[m])(lambda m=m: p2(m))
        at(t3[m])(lambda m=m: p2r(m))
        at(t3[m] + 3.9)(lambda m=m: d2d(m))
        at(t3[m] + 5.6)(lambda m=m: compute(m))

    for _, _, f in sorted(events, key=lambda e: e[:2]):
        f()

    def norm(i, carry):
        rows = pl.ds(pl.multiple_of(i * 16, 16), 16)
        v = CV[rows, :]
        mean = jnp.mean(v, axis=-1, keepdims=True)
        cen = v - mean
        var = jnp.mean(cen * cen, axis=-1, keepdims=True)
        n = cen * lax.rsqrt(var + 1e-05) * gain[...] + bias[...]
        ACT[rows, :] = (n * jax.nn.sigmoid(n)).astype(jnp.bfloat16)
        return carry

    lax.fori_loop(0, 8, norm, 0)

    for s in range(9):
        for d in st["od", s]:
            d.wait_recv()

    def project(j, carry):
        acc = None
        zs = pl.ds(j * 4, 4)
        for i in range(4):
            w = jnp.concatenate([O[i, 0, zs].reshape(512, 128), O[i, 1, zs].reshape(512, 128)], axis=1)
            part = lax.dot_general(
                ACT[:, 256 * i : 256 * i + 256], w, NT, preferred_element_type=jnp.float32
            )
            acc = part if acc is None else acc + part
        out[:, pl.ds(pl.multiple_of(j * 512, 512), 512)] = acc.astype(jnp.bfloat16)
        return carry

    lax.fori_loop(0, 4, project, 0)

    for d in sends:
        d.wait_send()

    @pl.when(sp < 63)
    def _():
        halo_r.wait_send()

    @pl.when(sp > 0)
    def _():
        halo_l.wait_send()


def on_device(tokens, w_value, w_gate, w_out, conv_taps, norm_gain, norm_bias):
    hbm = pl.BlockSpec(memory_space=pl.ANY)
    vmem = pl.BlockSpec(memory_space=pltpu.VMEM)
    mixed = pl.pallas_call(
        kernel,
        out_shape=jax.ShapeDtypeStruct((128, 2048), jnp.bfloat16),
        in_specs=[hbm] * 4 + [vmem] * 3,
        out_specs=vmem,
        scratch_shapes=[
            pltpu.VMEM((4, 2, 4, 4, 4, 2, 16, 256), jnp.bfloat16),
            pltpu.VMEM((4, 2, 16, 4, 32, 128), jnp.bfloat16),
            pltpu.VMEM((160, 2048), jnp.bfloat16),
            pltpu.VMEM((31, 1024), jnp.float32),
            pltpu.VMEM((128, 1024), jnp.float32),
            pltpu.VMEM((128, 1024), jnp.bfloat16),
            pltpu.SemaphoreType.DMA((NSEM,)),
            pltpu.SemaphoreType.DMA((NSEM,)),
            pltpu.SemaphoreType.DMA((4,)),
        ],
        compiler_params=pltpu.CompilerParams(
            collective_id=0, has_side_effects=True, vmem_limit_bytes=48 * 1024 * 1024
        ),
    )(
        tokens[0],
        w_value.T,
        w_gate.T,
        w_out.T,
        conv_taps.T,
        norm_gain[None, :],
        norm_bias[None, :],
    )
    return mixed[None]


def solution(mesh):
    in_specs = (P("dp", "sp", None), P("dp", "sp"), P("dp", "sp"), P("dp", "sp"), P(), P(), P())
    out_specs = P("dp", "sp", None)
    return jax.shard_map(
        on_device, mesh=mesh, in_specs=in_specs, out_specs=out_specs, check_vma=False
    )
```

```python
import jax
import jax.numpy as jnp
from jax import lax
from jax.experimental import pallas as pl
from jax.experimental.pallas import tpu as pltpu
from jax.sharding import PartitionSpec as P

MESH = pl.DeviceIdType.MESH
NSEM = 100
ORDER = [
    "ox", "s1", "halo", "oxr+", "oxr-", "oy", "p1_0", "s1l", "s1r", "oyr+", "oyr-", "p1rA0+", "p1rA0-",
    "p1rB0+", "p1rB0-", "g0", "p2A_0", "p1_1", "s1rr", "p2B_0", "p1_2", "p1rA1+", "g1_0", "p2rA0+", "g1_1",
    "p1rB1+", "p1rB1-", "g1_3", "p2rA0-", "p2rB0+", "p1rA2-", "p1rA2+", "p1rB2+", "g1_2", "g2_0", "p1rA1-",
    "p1rB2-", "p1_3", "g2_3", "p2B_1", "g2_1", "dA_0", "g2_2", "p2A_2", "g3_0", "p2rB0-", "g3_3", "p1rA3-",
    "p2B_2", "p2A_1", "g3_1", "p1rA3+", "p2rB1-", "g3_2", "p1rB3+", "p1rB3-", "g4_0", "dB_0", "g4_3",
    "p2rA2+", "p2rB1+", "p2A_3", "g4_1", "p2rA1+", "p2rA1-", "g4_2", "p2B_3", "p2rB2-", "g5_3", "g5_0",
    "p2rA2-", "g5_1", "p2rB2+", "p2rA3-", "p2rA3+", "g5_2", "p2rB3+", "p2rB3-", "c_0", "dB_1", "dA_1", "g6_3",
    "g6_0", "dA_2", "g6_1", "dB_2", "g6_2", "dA_3", "dB_3", "g7_3", "c_1", "g7_0", "g7_1", "c_2", "g7_2",
    "g8_3", "c_3", "g8_1", "g8_0", "g8_2",
]
SENDS = {"ox+": "ox", "ox-": "ox", "oxr": "ox", "oy+": "oy", "oy-": "oy", "oyr": "oy",
         "s1+": "s1", "s1-": "s1", "s1r": "s1", "od": "od"}
FIRST = 0
NT = (((1,), (1,)), ((), ()))


def kernel(
    tok, wv, wg, wo, taps_in, gain_in, bias_in, result,
    out, W, O, X, TB, T, gain, bias, CV, ACT, ssem, rsem, lsem,
):
    sp = lax.axis_index("sp")
    dp = lax.axis_index("dp")
    z, y = sp // 4, lax.rem(sp, 4)
    x, c = dp // 2, lax.rem(dp, 2)
    q, r = z // 4, lax.rem(z, 4)

    def dev(x=x, y=y, z=z, c=c):
        return {"sp": z * 4 + y, "dp": x * 2 + c}

    def mod(v, n):
        return lax.rem(v + n, n)

    xl, xr = mod(x - 1, 4), mod(x + 1, 4)
    yl, yr = mod(y - 1, 4), mod(y + 1, 4)
    zl, zr = mod(z - 1, 16), mod(z + 1, 16)
    z4l, z4r = mod(z - 4, 16), mod(z + 4, 16)
    peers = [q * 4 + mod(r + d, 4) for d in (1, 2, 3)]
    qs = [q, mod(q - 1, 4), mod(q + 1, 4), mod(q + 2, 4)]
    prev, nxt = mod(sp - 1, 64), mod(sp + 1, 64)

    local = [
        pltpu.make_async_copy(wv, W.at[x, c, q, r, y, 0], lsem.at[0]),
        pltpu.make_async_copy(wg, W.at[x, c, q, r, y, 1], lsem.at[1]),
        pltpu.make_async_copy(wo, O.at[x, c, z, y], lsem.at[2]),
        pltpu.make_async_copy(tok, X.at[pl.ds(16, 128)], lsem.at[3]),
        pltpu.make_async_copy(taps_in, TB, lsem.at[4]),
        pltpu.make_async_copy(gain_in, gain, lsem.at[5]),
        pltpu.make_async_copy(bias_in, bias, lsem.at[6]),
    ]
    for d in local:
        d.start()

    barrier = pltpu.get_barrier_semaphore()
    partners = [dev(x=xl), dev(x=xr), dev(y=yl), dev(y=yr), dev(z=zl), dev(z=zr), dev(z=z4l), dev(z=z4r)]
    partners += [dev(z=p) for p in peers]
    partners += [dev(c=1 - c), {"sp": prev, "dp": dp}, {"sp": nxt, "dp": dp}]
    for p in partners:
        pl.semaphore_signal(barrier, inc=1, device_id=p, device_id_type=MESH)

    @pl.when(sp == 0)
    def _():
        X[pl.ds(0, 16), :] = jnp.zeros((16, 2048), jnp.bfloat16)

    @pl.when(sp == 63)
    def _():
        X[pl.ds(144, 16), :] = jnp.zeros((16, 2048), jnp.bfloat16)

    with jax.named_scope("barrier"):
        for d in local:
            d.wait()
        pl.semaphore_wait(barrier, len(partners))

    groups = {}

    kinds = {}

    def describe(src, dst, to, key, kind):
        i = groups.setdefault(key, len(groups))
        j = kinds.setdefault(kind, len(kinds))
        return pltpu.make_async_remote_copy(
            src_ref=src, dst_ref=dst, send_sem=ssem.at[j], recv_sem=rsem.at[i],
            device_id=to, device_id_type=MESH,
        )

    def send(key, ref, to):
        kind = key[0] if isinstance(key, tuple) else SENDS[key]
        describe(ref, ref, to, key, kind).start()

    def arrived(key, ref):
        describe(ref, ref, dev(c=1 - c), key, "d2d").wait_recv()

    def sent(kind, ref):
        describe(ref, ref, dev(c=1 - c), "od", kind).wait_send()

    events = {}

    def event(name):
        def add(f):
            events[name] = f
        return add

    halo_r = describe(X.at[pl.ds(128, 16)], X.at[pl.ds(0, 16)], {"sp": nxt, "dp": dp}, "hr", "hr")
    halo_l = describe(X.at[pl.ds(16, 16)], X.at[pl.ds(144, 16)], {"sp": prev, "dp": dp}, "hl", "hl")
    lo, hi = pl.ds(0, 2), pl.ds(2, 2)

    @event("halo")
    def _():
        @pl.when(sp < 63)
        def _():
            halo_r.start()

        @pl.when(sp > 0)
        def _():
            halo_l.start()

        T[...] = TB[...].astype(jnp.float32)

    @event("ox")
    def _():
        send("ox+", O.at[x, c, z, y], dev(x=xr))
        send("ox-", O.at[x, c, z, y], dev(x=xl))

    @event("oxr+")
    def _():
        arrived("ox+", O.at[x, c, z, y])
        send("oxr", O.at[xl, c, z, y, pl.ds(0, 16)], dev(x=xr))

    @event("oxr-")
    def _():
        arrived("ox-", O.at[x, c, z, y])
        send("oxr", O.at[xr, c, z, y, pl.ds(16, 16)], dev(x=xl))

    @event("oy")
    def _():
        arrived("oxr", O.at[x, c, z, y])
        send("oy+", O.at[:, c, z, y], dev(y=yr))
        send("oy-", O.at[:, c, z, y], dev(y=yl))

    @event("oyr+")
    def _():
        arrived("oy+", O.at[:, c, z, y])
        send("oyr", O.at[lo, c, z, yl], dev(y=yr))

    @event("oyr-")
    def _():
        arrived("oy-", O.at[:, c, z, y])
        send("oyr", O.at[hi, c, z, yr], dev(y=yl))

    stepped = [0] * 9

    def ring(s, h):
        zo, zp = mod(z - s, 16), mod(z + s, 16)
        if s > 0:
            arrived(("ring", s - 1, h), O.at[:, c, z, pl.ds(0, 2 if s < 8 else 1)])
        if s < 8:
            send(("ring", s, h), O.at[:, c, zo, h], dev(z=zr))
        if s < 7:
            send(("ring", s, h), O.at[:, c, zp, h], dev(z=zl))
        stepped[s] += 1
        if stepped[s] == 4:
            send("od", O.at[:, c, zo], dev(c=1 - c))
            if 0 < s < 8:
                send("od", O.at[:, c, zp], dev(c=1 - c))

    @event("g0")
    def _():
        arrived("oyr", O.at[:, c, z, y])
        for h in range(4):
            ring(0, h)

    for s in range(1, 9):
        for h in range(4):
            event(f"g{s}_{h}")(lambda s=s, h=h: ring(s, h))

    def s2(m):
        for p in peers:
            send(("s2", m), W.at[x, c, qs[m], r, y], dev(z=p))

    @event("s1")
    def _():
        s2(0)
        send("s1+", W.at[x, c, q, r, y], dev(z=z4r))
        send("s1-", W.at[x, c, q, r, y], dev(z=z4l))

    @event("s1l")
    def _():
        arrived("s1+", W.at[x, c, q, r, y])
        send("s1r", W.at[x, c, qs[1], r, y, 0], dev(z=z4r))
        s2(1)

    @event("s1r")
    def _():
        arrived("s1-", W.at[x, c, q, r, y])
        send("s1r", W.at[x, c, qs[2], r, y, 1], dev(z=z4l))
        s2(2)

    @event("s1rr")
    def _():
        arrived("s1r", W.at[x, c, q, r, y])
        s2(3)

    yn, xn = {"+": dev(y=yr), "-": dev(y=yl)}, {"+": dev(x=xr), "-": dev(x=xl)}
    at = {"o": 0, "+": -1, "-": 1, "x": 2}

    def part(T, m, p, rows=slice(None)):
        if T == "A":
            return W.at[x, c, qs[m], rows, mod(y + at[p], 4), 0]
        return W.at[mod(x + at[p], 4), c, qs[m], rows, y, 1]

    def slab(T, m, d, rows=slice(None)):
        if T == "A":
            return W.at[mod(x + at[d], 4), c, qs[m], rows, :, 0]
        return W.at[:, c, qs[m], rows, mod(y + at[d], 4), 1]

    ring1, ring2 = {"A": yn, "B": xn}, {"A": xn, "B": yn}
    half = {"+": lo, "-": hi}

    def p1(m):
        arrived(("s2", m), W.at[x, c, qs[m], pl.ds(0, 3), y])
        for T in "AB":
            for d in "+-":
                send(("p1", T, m, d), part(T, m, "o"), ring1[T][d])
            for d in "+-":
                send(("p2", T, m, d), part(T, m, "o"), ring2[T][d])

    def p1r(T, m, d):
        arrived(("p1", T, m, d), part(T, m, "o"))
        send(("p1r", T, m), part(T, m, d, half[d]), ring1[T][d])
        for e in "+-":
            send(("p2", T, m, e), part(T, m, d), ring2[T][e])

    def p2(T, m):
        arrived(("p1r", T, m), part(T, m, "o"))
        for e in "+-":
            send(("p2", T, m, e), part(T, m, "x"), ring2[T][e])
        send(("d2d", m), slab(T, m, "o"), dev(c=1 - c))

    def p2r(T, m, d):
        arrived(("p2", T, m, d), slab(T, m, d))
        send(("p2r", T, m), slab(T, m, d, half[d]), ring2[T][d])
        send(("d2d", m), slab(T, m, d), dev(c=1 - c))

    def d2d(T, m):
        arrived(("p2r", T, m), slab(T, m, "+"))
        send(("d2d", m), slab(T, m, "x"), dev(c=1 - c))

    def compute(m):
        arrived(("d2d", m), W.at[:, 1 - c, qs[m]])
        if m == FIRST:
            @pl.when(sp > 0)
            def _():
                halo_r.wait_recv()

            @pl.when(sp < 63)
            def _():
                halo_l.wait_recv()

        qm = qs[m]
        acc = [None, None]
        for i in range(8):
            xs = X[:, 256 * i : 256 * i + 256]
            for k in (0, 1):
                w = W[i // 2, i % 2, qm, :, :, k].reshape(256, 256)
                part = lax.dot_general(xs, w, NT, preferred_element_type=jnp.float32)
                acc[k] = part if acc[k] is None else acc[k] + part
        gated = (acc[0] * jax.nn.sigmoid(acc[1])).astype(jnp.bfloat16).astype(jnp.float32)
        for h in (0, 1):
            strip = gated[:, 128 * h : 128 * h + 128]
            lanes = pl.ds(pl.multiple_of(qm * 256 + 128 * h, 128), 128)
            total = jnp.zeros((128, 128), jnp.float32)
            for shift in range(8):
                rolled = strip if shift == 0 else pltpu.roll(strip, 160 - shift, 0)
                for k in range(31):
                    if (k + 1) % 8 == shift:
                        first = (k + 1) // 8 * 8
                        total = total + T[pl.ds(k, 1), lanes] * rolled[first : first + 128]
            CV[:, lanes] = total.astype(jnp.bfloat16).astype(jnp.float32)

    for m in range(4):
        event(f"p1_{m}")(lambda m=m: p1(m))
        event(f"c_{m}")(lambda m=m: compute(m))
        for T_ in "AB":
            event(f"p2{T_}_{m}")(lambda m=m, T_=T_: p2(T_, m))
            event(f"d{T_}_{m}")(lambda m=m, T_=T_: d2d(T_, m))
            for d in "+-":
                event(f"p1r{T_}{m}{d}")(lambda m=m, T_=T_, d=d: p1r(T_, m, d))
                event(f"p2r{T_}{m}{d}")(lambda m=m, T_=T_, d=d: p2r(T_, m, d))

    for name in ORDER:
        with jax.named_scope(name):
            events[name]()

    assert len(groups) == NSEM and len(kinds) == 13, (len(groups), len(kinds))

    def norm(i, carry):
        rows = pl.ds(pl.multiple_of(i * 16, 16), 16)
        v = CV[rows, :]
        mean = jnp.mean(v, axis=-1, keepdims=True)
        cen = v - mean
        var = jnp.mean(cen * cen, axis=-1, keepdims=True)
        n = cen * lax.rsqrt(var + 1e-05) * gain[...] + bias[...]
        ACT[rows, :] = (n * jax.nn.sigmoid(n)).astype(jnp.bfloat16)
        return carry

    with jax.named_scope("norm"):
        lax.fori_loop(0, 8, norm, 0)

    with jax.named_scope("out_rows"):
        arrived("od", O.at[:, 1 - c])

    def emit(j):
        cols = pl.ds(pl.multiple_of(j * 512, 512), 512)
        return pltpu.make_async_copy(out.at[:, cols], result.at[:, cols], lsem.at[7 + j])

    def project(j, carry):
        acc = None
        zs = pl.ds(j * 4, 4)
        for i in range(4):
            w = jnp.concatenate([O[i, 0, zs].reshape(512, 128), O[i, 1, zs].reshape(512, 128)], axis=1)
            part = lax.dot_general(
                ACT[:, 256 * i : 256 * i + 256], w, NT, preferred_element_type=jnp.float32
            )
            acc = part if acc is None else acc + part
        out[:, pl.ds(pl.multiple_of(j * 512, 512), 512)] = acc.astype(jnp.bfloat16)
        emit(j).start()
        return carry

    with jax.named_scope("project"):
        lax.fori_loop(0, 4, project, 0)
    with jax.named_scope("outdma"):
        for j in range(4):
            emit(j).wait()

    with jax.named_scope("drain"):
        sent("p2", W.at[pl.ds(0, 2), c])
        sent("p2r", W.at[0, c])
        sent("p1", W.at[0, c, pl.ds(0, 2)])
        sent("p1r", W.at[0, c, 0])
        sent("d2d", W.at[:, c])
        sent("s2", W.at[0, c, 0, pl.ds(0, 3)])
        sent("s1", W.at[0, c, 0, pl.ds(0, 3), 0])
        sent("ox", O.at[0, c, 0, pl.ds(0, 3)])
        sent("oy", O.at[pl.ds(0, 3), c, 0])
        sent("ring", O.at[:, c, pl.ds(0, 15)])
        sent("od", O.at[:, c])

    @pl.when(sp < 63)
    def _():
        halo_r.wait_send()

    @pl.when(sp > 0)
    def _():
        halo_l.wait_send()


def on_device(tokens, w_value, w_gate, w_out, conv_taps, norm_gain, norm_bias):
    hbm = pl.BlockSpec(memory_space=pltpu.HBM)
    vmem = pl.BlockSpec(memory_space=pltpu.VMEM)
    mixed = pl.pallas_call(
        kernel,
        out_shape=jax.ShapeDtypeStruct((128, 2048), jnp.bfloat16),
        in_specs=[hbm] * 7,
        out_specs=hbm,
        scratch_shapes=[
            pltpu.VMEM((128, 2048), jnp.bfloat16),
            pltpu.VMEM((4, 2, 4, 4, 4, 2, 16, 256), jnp.bfloat16),
            pltpu.VMEM((4, 2, 16, 4, 32, 128), jnp.bfloat16),
            pltpu.VMEM((160, 2048), jnp.bfloat16),
            pltpu.VMEM((31, 1024), jnp.bfloat16),
            pltpu.VMEM((31, 1024), jnp.float32),
            pltpu.VMEM((1, 1024), jnp.float32),
            pltpu.VMEM((1, 1024), jnp.float32),
            pltpu.VMEM((128, 1024), jnp.float32),
            pltpu.VMEM((128, 1024), jnp.bfloat16),
            pltpu.SemaphoreType.DMA((13,)),
            pltpu.SemaphoreType.DMA((NSEM,)),
            pltpu.SemaphoreType.DMA((11,)),
        ],
        compiler_params=pltpu.CompilerParams(
            collective_id=0, has_side_effects=True, vmem_limit_bytes=67043328
        ),
    )(
        tokens[0],
        w_value.T,
        w_gate.T,
        w_out.T,
        conv_taps.T,
        norm_gain[None, :],
        norm_bias[None, :],
    )
    return mixed[None]


def solution(mesh):
    in_specs = (P("dp", "sp", None), P("dp", "sp"), P("dp", "sp"), P("dp", "sp"), P(), P(), P())
    out_specs = P("dp", "sp", None)
    return jax.shard_map(
        on_device, mesh=mesh, in_specs=in_specs, out_specs=out_specs, check_vma=False
    )
```

```python
import jax
import jax.numpy as jnp
from jax import lax
from jax.experimental import pallas as pl
from jax.experimental.pallas import tpu as pltpu
from jax.sharding import PartitionSpec as P

MESH = pl.DeviceIdType.MESH
NSEM = 96
ORDER = [
    "s1", "ox", "halo", "oy", "p1_0", "s1l", "s1r", "p1rA0-", "g0", "p1rA0+", "s1rr", "p1rB0+", "p2A_0",
    "p1rB0-", "p2B_0", "p1_1", "g1_0", "g1_1", "p1_2", "g1_3", "g1_2", "p2rA0-", "p2rA0+", "p1rB1+", "g2_0",
    "p2rB0-", "p1rA1+", "p1rA1-", "g2_1", "p1_3", "p1rB2+", "p1rB1-", "g2_3", "g2_2", "p1rA2-", "p1rA2+",
    "p1rB2-", "g3_0", "p2rB0+", "g3_1", "g3_3", "p1rA3+", "p2A_1", "g3_2", "dA_0", "p2B_1", "p1rA3-", "g4_0",
    "g4_1", "p1rB3+", "p1rB3-", "g4_3", "g4_2", "p2A_2", "p2B_2", "g5_0", "p2rA1+", "p2rA1-", "g5_1",
    "p2rB1+", "p2A_3", "p2rB1-", "dB_0", "p2B_3", "g5_3", "g5_2", "g6_0", "p2rB2+", "p2rB2-", "p2rA2-",
    "g6_1", "p2rA2+", "p2rA3+", "p2rA3-", "g6_3", "p2rB3+", "g6_2", "p2rB3-", "dA_1", "c_0", "g7_0", "dB_1",
    "g7_1", "dB_2", "dA_2", "g7_3", "g7_2", "dA_3", "dB_3", "c_1", "c_2", "g8_1", "g8_3", "g8_0", "g8_2",
    "c_3",
]
SENDS = {"ox": "ox", "oy": "oy",
         "s1+": "s1", "s1-": "s1", "s1r": "s1", "od": "od"}
FIRST = 0
DIRECT = (0,)
NT = (((1,), (1,)), ((), ()))


def kernel(
    tok, wv, wg, wo, taps_in, gain_in, bias_in, result,
    out, W, O, X, TB, T, gain, bias, CV, ACT, ssem, rsem, lsem,
):
    sp = lax.axis_index("sp")
    dp = lax.axis_index("dp")
    z, y = sp // 4, lax.rem(sp, 4)
    x, c = dp // 2, lax.rem(dp, 2)
    q, r = z // 4, lax.rem(z, 4)

    def dev(x=x, y=y, z=z, c=c):
        return {"sp": z * 4 + y, "dp": x * 2 + c}

    def mod(v, n):
        return lax.rem(v + n, n)

    xl, xr = mod(x - 1, 4), mod(x + 1, 4)
    yl, yr = mod(y - 1, 4), mod(y + 1, 4)
    zl, zr = mod(z - 1, 16), mod(z + 1, 16)
    z4l, z4r = mod(z - 4, 16), mod(z + 4, 16)
    peers = [q * 4 + mod(r + d, 4) for d in (1, 2, 3)]
    qs = [q, mod(q - 1, 4), mod(q + 1, 4), mod(q + 2, 4)]
    prev, nxt = mod(sp - 1, 64), mod(sp + 1, 64)

    local = [
        pltpu.make_async_copy(wv, W.at[x, c, q, r, y, 0], lsem.at[0]),
        pltpu.make_async_copy(wg, W.at[x, c, q, r, y, 1], lsem.at[1]),
        pltpu.make_async_copy(wo, O.at[x, c, z, y], lsem.at[2]),
        pltpu.make_async_copy(tok, X.at[pl.ds(16, 128)], lsem.at[3]),
        pltpu.make_async_copy(taps_in, TB, lsem.at[4]),
        pltpu.make_async_copy(gain_in, gain, lsem.at[5]),
        pltpu.make_async_copy(bias_in, bias, lsem.at[6]),
    ]
    for d in local:
        d.start()

    barrier = pltpu.get_barrier_semaphore()
    partners = [dev(x=xl), dev(x=xr), dev(y=yl), dev(y=yr), dev(z=zl), dev(z=zr), dev(z=z4l), dev(z=z4r)]
    partners += [dev(z=p) for p in peers]
    partners += [dev(x=mod(x + 2, 4)), dev(y=mod(y + 2, 4))]
    partners += [dev(c=1 - c), {"sp": prev, "dp": dp}, {"sp": nxt, "dp": dp}]
    for p in partners:
        pl.semaphore_signal(barrier, inc=1, device_id=p, device_id_type=MESH)

    @pl.when(sp == 0)
    def _():
        X[pl.ds(0, 16), :] = jnp.zeros((16, 2048), jnp.bfloat16)

    @pl.when(sp == 63)
    def _():
        X[pl.ds(144, 16), :] = jnp.zeros((16, 2048), jnp.bfloat16)

    with jax.named_scope("barrier"):
        for d in local:
            d.wait()
        pl.semaphore_wait(barrier, len(partners))

    groups = {}

    kinds = {}

    def describe(src, dst, to, key, kind):
        i = groups.setdefault(key, len(groups))
        j = kinds.setdefault(kind, len(kinds))
        return pltpu.make_async_remote_copy(
            src_ref=src, dst_ref=dst, send_sem=ssem.at[j], recv_sem=rsem.at[i],
            device_id=to, device_id_type=MESH,
        )

    def send(key, ref, to):
        kind = key[0] if isinstance(key, tuple) else SENDS[key]
        describe(ref, ref, to, key, kind).start()

    def arrived(key, ref):
        describe(ref, ref, dev(c=1 - c), key, "d2d").wait_recv()

    def sent(kind, ref):
        describe(ref, ref, dev(c=1 - c), "od", kind).wait_send()

    events = {}

    def event(name):
        def add(f):
            events[name] = f
        return add

    halo_r = describe(X.at[pl.ds(128, 16)], X.at[pl.ds(0, 16)], {"sp": nxt, "dp": dp}, "hr", "hr")
    halo_l = describe(X.at[pl.ds(16, 16)], X.at[pl.ds(144, 16)], {"sp": prev, "dp": dp}, "hl", "hl")
    lo, hi = pl.ds(0, 2), pl.ds(2, 2)

    @event("halo")
    def _():
        @pl.when(sp < 63)
        def _():
            halo_r.start()

        @pl.when(sp > 0)
        def _():
            halo_l.start()

        T[...] = TB[...].astype(jnp.float32)

    @event("ox")
    def _():
        for d in (1, 3, 2):
            send("ox", O.at[x, c, z, y], dev(x=mod(x + d, 4)))

    @event("oy")
    def _():
        arrived("ox", O.at[pl.ds(0, 3), c, z, y])
        for d in (1, 3, 2):
            send("oy", O.at[:, c, z, y], dev(y=mod(y + d, 4)))

    stepped = [0] * 9

    def ring(s, h):
        zo, zp = mod(z - s, 16), mod(z + s, 16)
        if s > 0:
            arrived(("ring", s - 1, h), O.at[:, c, z, pl.ds(0, 2 if s < 8 else 1)])
        if s < 8:
            send(("ring", s, h), O.at[:, c, zo, h], dev(z=zr))
        if s < 7:
            send(("ring", s, h), O.at[:, c, zp, h], dev(z=zl))
        stepped[s] += 1
        if stepped[s] == 4:
            send("od", O.at[:, c, zo], dev(c=1 - c))
            if 0 < s < 8:
                send("od", O.at[:, c, zp], dev(c=1 - c))

    @event("g0")
    def _():
        arrived("oy", O.at[:, c, z, pl.ds(0, 3)])
        for h in range(4):
            ring(0, h)

    for s in range(1, 9):
        for h in range(4):
            event(f"g{s}_{h}")(lambda s=s, h=h: ring(s, h))

    def s2(m):
        for p in peers:
            send(("s2", m), W.at[x, c, qs[m], r, y], dev(z=p))

    @event("s1")
    def _():
        s2(0)
        send("s1+", W.at[x, c, q, r, y], dev(z=z4r))
        send("s1-", W.at[x, c, q, r, y], dev(z=z4l))

    @event("s1l")
    def _():
        arrived("s1+", W.at[x, c, q, r, y])
        send("s1r", W.at[x, c, qs[1], r, y, 0], dev(z=z4r))
        s2(1)

    @event("s1r")
    def _():
        arrived("s1-", W.at[x, c, q, r, y])
        send("s1r", W.at[x, c, qs[2], r, y, 1], dev(z=z4l))
        s2(2)

    @event("s1rr")
    def _():
        arrived("s1r", W.at[x, c, q, r, y])
        s2(3)

    yn, xn = {"+": dev(y=yr), "-": dev(y=yl)}, {"+": dev(x=xr), "-": dev(x=xl)}
    at = {"o": 0, "+": -1, "-": 1, "x": 2}

    def part(T, m, p, rows=slice(None)):
        if T == "A":
            return W.at[x, c, qs[m], rows, mod(y + at[p], 4), 0]
        return W.at[mod(x + at[p], 4), c, qs[m], rows, y, 1]

    def slab(T, m, d, rows=slice(None)):
        if T == "A":
            return W.at[mod(x + at[d], 4), c, qs[m], rows, :, 0]
        return W.at[:, c, qs[m], rows, mod(y + at[d], 4), 1]

    ring1, ring2 = {"A": yn, "B": xn}, {"A": xn, "B": yn}
    half = {"+": lo, "-": hi}

    def p1(m):
        arrived(("s2", m), W.at[x, c, qs[m], pl.ds(0, 3), y])
        for T in "AB":
            for d in "+-":
                send(("p1", T, m, d), part(T, m, "o"), ring1[T][d])
            for d in "+-":
                send(("p2", T, m, d), part(T, m, "o"), ring2[T][d])
            if m in DIRECT:
                send(("p1r", T, m), part(T, m, "o"), dev(y=mod(y + 2, 4)) if T == "A" else dev(x=mod(x + 2, 4)))

    def p1r(T, m, d):
        arrived(("p1", T, m, d), part(T, m, "o"))
        if m not in DIRECT:
            send(("p1r", T, m), part(T, m, d, half[d]), ring1[T][d])
        for e in "+-":
            send(("p2", T, m, e), part(T, m, d), ring2[T][e])

    def p2(T, m):
        arrived(("p1r", T, m), part(T, m, "o"))
        for e in "+-":
            send(("p2", T, m, e), part(T, m, "x"), ring2[T][e])
        send(("d2d", m), slab(T, m, "o"), dev(c=1 - c))

    def p2r(T, m, d):
        arrived(("p2", T, m, d), slab(T, m, d))
        send(("p2r", T, m), slab(T, m, d, half[d]), ring2[T][d])
        send(("d2d", m), slab(T, m, d), dev(c=1 - c))

    def d2d(T, m):
        arrived(("p2r", T, m), slab(T, m, "+"))
        send(("d2d", m), slab(T, m, "x"), dev(c=1 - c))

    def compute(m):
        arrived(("d2d", m), W.at[:, 1 - c, qs[m]])
        if m == FIRST:
            @pl.when(sp > 0)
            def _():
                halo_r.wait_recv()

            @pl.when(sp < 63)
            def _():
                halo_l.wait_recv()

        qm = qs[m]
        acc = [None, None]
        for i in range(8):
            xs = X[:, 256 * i : 256 * i + 256]
            for k in (0, 1):
                w = W[i // 2, i % 2, qm, :, :, k].reshape(256, 256)
                part = lax.dot_general(xs, w, NT, preferred_element_type=jnp.float32)
                acc[k] = part if acc[k] is None else acc[k] + part
        gated = (acc[0] * jax.nn.sigmoid(acc[1])).astype(jnp.bfloat16).astype(jnp.float32)
        for h in (0, 1):
            strip = gated[:, 128 * h : 128 * h + 128]
            lanes = pl.ds(pl.multiple_of(qm * 256 + 128 * h, 128), 128)
            total = jnp.zeros((128, 128), jnp.float32)
            for shift in range(8):
                rolled = strip if shift == 0 else pltpu.roll(strip, 160 - shift, 0)
                for k in range(31):
                    if (k + 1) % 8 == shift:
                        first = (k + 1) // 8 * 8
                        total = total + T[pl.ds(k, 1), lanes] * rolled[first : first + 128]
            CV[:, lanes] = total.astype(jnp.bfloat16).astype(jnp.float32)

    for m in range(4):
        event(f"p1_{m}")(lambda m=m: p1(m))
        event(f"c_{m}")(lambda m=m: compute(m))
        for T_ in "AB":
            event(f"p2{T_}_{m}")(lambda m=m, T_=T_: p2(T_, m))
            event(f"d{T_}_{m}")(lambda m=m, T_=T_: d2d(T_, m))
            for d in "+-":
                event(f"p1r{T_}{m}{d}")(lambda m=m, T_=T_, d=d: p1r(T_, m, d))
                event(f"p2r{T_}{m}{d}")(lambda m=m, T_=T_, d=d: p2r(T_, m, d))

    for name in ORDER:
        with jax.named_scope(name):
            events[name]()

    assert len(groups) == NSEM and len(kinds) == 13, (len(groups), len(kinds))

    def norm(i, carry):
        rows = pl.ds(pl.multiple_of(i * 16, 16), 16)
        v = CV[rows, :]
        mean = jnp.mean(v, axis=-1, keepdims=True)
        cen = v - mean
        var = jnp.mean(cen * cen, axis=-1, keepdims=True)
        n = cen * lax.rsqrt(var + 1e-05) * gain[...] + bias[...]
        ACT[rows, :] = (n * jax.nn.sigmoid(n)).astype(jnp.bfloat16)
        return carry

    with jax.named_scope("norm"):
        lax.fori_loop(0, 8, norm, 0)

    with jax.named_scope("out_rows"):
        arrived("od", O.at[:, 1 - c])

    def emit(j):
        cols = pl.ds(pl.multiple_of(j * 512, 512), 512)
        return pltpu.make_async_copy(out.at[:, cols], result.at[:, cols], lsem.at[7 + j])

    def project(j, carry):
        acc = None
        zs = pl.ds(j * 4, 4)
        for i in range(4):
            w = jnp.concatenate([O[i, 0, zs].reshape(512, 128), O[i, 1, zs].reshape(512, 128)], axis=1)
            part = lax.dot_general(
                ACT[:, 256 * i : 256 * i + 256], w, NT, preferred_element_type=jnp.float32
            )
            acc = part if acc is None else acc + part
        out[:, pl.ds(pl.multiple_of(j * 512, 512), 512)] = acc.astype(jnp.bfloat16)
        emit(j).start()
        return carry

    with jax.named_scope("project"):
        lax.fori_loop(0, 4, project, 0)
    with jax.named_scope("outdma"):
        for j in range(4):
            emit(j).wait()

    with jax.named_scope("drain"):
        sent("p2", W.at[pl.ds(0, 2), c])
        sent("p2r", W.at[0, c])
        sent("p1", W.at[0, c, pl.ds(0, 2)])
        sent("p1r", W.at[0, c, 0])
        sent("d2d", W.at[:, c])
        sent("s2", W.at[0, c, 0, pl.ds(0, 3)])
        sent("s1", W.at[0, c, 0, pl.ds(0, 3), 0])
        sent("ox", O.at[0, c, 0, pl.ds(0, 3)])
        sent("oy", O.at[pl.ds(0, 3), c, 0])
        sent("ring", O.at[:, c, pl.ds(0, 15)])
        sent("od", O.at[:, c])

    @pl.when(sp < 63)
    def _():
        halo_r.wait_send()

    @pl.when(sp > 0)
    def _():
        halo_l.wait_send()


def on_device(tokens, w_value, w_gate, w_out, conv_taps, norm_gain, norm_bias):
    hbm = pl.BlockSpec(memory_space=pltpu.HBM)
    vmem = pl.BlockSpec(memory_space=pltpu.VMEM)
    mixed = pl.pallas_call(
        kernel,
        out_shape=jax.ShapeDtypeStruct((128, 2048), jnp.bfloat16),
        in_specs=[hbm] * 7,
        out_specs=hbm,
        scratch_shapes=[
            pltpu.VMEM((128, 2048), jnp.bfloat16),
            pltpu.VMEM((4, 2, 4, 4, 4, 2, 16, 256), jnp.bfloat16),
            pltpu.VMEM((4, 2, 16, 4, 32, 128), jnp.bfloat16),
            pltpu.VMEM((160, 2048), jnp.bfloat16),
            pltpu.VMEM((31, 1024), jnp.bfloat16),
            pltpu.VMEM((31, 1024), jnp.float32),
            pltpu.VMEM((1, 1024), jnp.float32),
            pltpu.VMEM((1, 1024), jnp.float32),
            pltpu.VMEM((128, 1024), jnp.float32),
            pltpu.VMEM((128, 1024), jnp.bfloat16),
            pltpu.SemaphoreType.DMA((13,)),
            pltpu.SemaphoreType.DMA((NSEM,)),
            pltpu.SemaphoreType.DMA((11,)),
        ],
        compiler_params=pltpu.CompilerParams(
            collective_id=0, has_side_effects=True, vmem_limit_bytes=67043328
        ),
    )(
        tokens[0],
        w_value.T,
        w_gate.T,
        w_out.T,
        conv_taps.T,
        norm_gain[None, :],
        norm_bias[None, :],
    )
    return mixed[None]


def solution(mesh):
    in_specs = (P("dp", "sp", None), P("dp", "sp"), P("dp", "sp"), P("dp", "sp"), P(), P(), P())
    out_specs = P("dp", "sp", None)
    return jax.shard_map(
        on_device, mesh=mesh, in_specs=in_specs, out_specs=out_specs, check_vma=False
    )
```

```python
import jax
import jax.numpy as jnp
from jax import lax
from jax.experimental import pallas as pl
from jax.experimental.pallas import tpu as pltpu
from jax.sharding import PartitionSpec as P

MESH = pl.DeviceIdType.MESH
NSEM = 96
ORDER = [
    "s1", "ox", "halo", "oy", "p1_0", "s1l", "s1r", "p1rA0-", "g0", "p1rA0+", "s1rr", "p1rB0+", "p2A_0",
    "p1rB0-", "p2B_0", "p1_1", "g1_0", "g1_1", "p1_2", "g1_3", "g1_2", "p2rA0-", "p2rA0+", "p1rB1+", "g2_0",
    "p2rB0-", "p1rA1+", "p1rA1-", "g2_1", "p1_3", "p1rB2+", "p1rB1-", "g2_3", "g2_2", "p1rA2-", "p1rA2+",
    "p1rB2-", "g3_0", "p2rB0+", "g3_1", "g3_3", "p1rA3+", "p2A_1", "g3_2", "dA_0", "p2B_1", "p1rA3-", "g4_0",
    "g4_1", "p1rB3+", "p1rB3-", "g4_3", "g4_2", "p2A_2", "p2B_2", "g5_0", "p2rA1+", "p2rA1-", "g5_1",
    "p2rB1+", "p2A_3", "p2rB1-", "dB_0", "p2B_3", "g5_3", "g5_2", "g6_0", "p2rB2+", "p2rB2-", "p2rA2-",
    "g6_1", "dA_1", "dB_1", "p2rA2+", "p2rA3+", "p2rA3-", "g6_3", "p2rB3+", "g6_2", "p2rB3-", "c_0", "g7_0",
    "g7_1", "dB_2", "dA_2", "g7_3", "g7_2", "dA_3", "dB_3", "c_1", "c_2", "g8_1", "g8_3", "g8_0", "g8_2",
    "c_3",
]
SENDS = {"ox": "ox", "oy": "oy",
         "s1+": "s1", "s1-": "s1", "s1r": "s1", "od": "od"}
FIRST = 0
DIRECT = (0,)
NT = (((1,), (1,)), ((), ()))


def kernel(
    tok, wv, wg, wo, taps_in, gain_in, bias_in, out,
    W, O, X, TB, T, gain, bias, CV, ACT, ssem, rsem, lsem,
):
    sp = lax.axis_index("sp")
    dp = lax.axis_index("dp")
    z, y = sp // 4, lax.rem(sp, 4)
    x, c = dp // 2, lax.rem(dp, 2)
    q, r = z // 4, lax.rem(z, 4)

    def dev(x=x, y=y, z=z, c=c):
        return {"sp": z * 4 + y, "dp": x * 2 + c}

    def mod(v, n):
        return lax.rem(v + n, n)

    xl, xr = mod(x - 1, 4), mod(x + 1, 4)
    yl, yr = mod(y - 1, 4), mod(y + 1, 4)
    zl, zr = mod(z - 1, 16), mod(z + 1, 16)
    z4l, z4r = mod(z - 4, 16), mod(z + 4, 16)
    peers = [q * 4 + mod(r + d, 4) for d in (1, 2, 3)]
    qs = [q, mod(q - 1, 4), mod(q + 1, 4), mod(q + 2, 4)]
    prev, nxt = mod(sp - 1, 64), mod(sp + 1, 64)

    local = [
        pltpu.make_async_copy(wv, W.at[x, c, q, r, y, 0], lsem.at[0]),
        pltpu.make_async_copy(wg, W.at[x, c, q, r, y, 1], lsem.at[1]),
        pltpu.make_async_copy(wo, O.at[x, c, z, y], lsem.at[2]),
        pltpu.make_async_copy(tok, X.at[pl.ds(16, 128)], lsem.at[3]),
        pltpu.make_async_copy(taps_in, TB, lsem.at[4]),
        pltpu.make_async_copy(gain_in, gain, lsem.at[5]),
        pltpu.make_async_copy(bias_in, bias, lsem.at[6]),
    ]
    for d in local:
        d.start()

    barrier = pltpu.get_barrier_semaphore()
    partners = [dev(x=xl), dev(x=xr), dev(y=yl), dev(y=yr), dev(z=zl), dev(z=zr), dev(z=z4l), dev(z=z4r)]
    partners += [dev(z=p) for p in peers]
    partners += [dev(x=mod(x + 2, 4)), dev(y=mod(y + 2, 4))]
    partners += [dev(c=1 - c), {"sp": prev, "dp": dp}, {"sp": nxt, "dp": dp}]
    for p in partners:
        pl.semaphore_signal(barrier, inc=1, device_id=p, device_id_type=MESH)

    @pl.when(sp == 0)
    def _():
        X[pl.ds(0, 16), :] = jnp.zeros((16, 2048), jnp.bfloat16)

    @pl.when(sp == 63)
    def _():
        X[pl.ds(144, 16), :] = jnp.zeros((16, 2048), jnp.bfloat16)

    with jax.named_scope("barrier"):
        for d in local:
            d.wait()
        pl.semaphore_wait(barrier, len(partners))

    groups = {}

    kinds = {}

    def describe(src, dst, to, key, kind):
        i = groups.setdefault(key, len(groups))
        j = kinds.setdefault(kind, len(kinds))
        return pltpu.make_async_remote_copy(
            src_ref=src, dst_ref=dst, send_sem=ssem.at[j], recv_sem=rsem.at[i],
            device_id=to, device_id_type=MESH,
        )

    def send(key, ref, to):
        kind = key[0] if isinstance(key, tuple) else SENDS[key]
        describe(ref, ref, to, key, kind).start()

    def arrived(key, ref):
        describe(ref, ref, dev(c=1 - c), key, "d2d").wait_recv()

    def sent(kind, ref):
        describe(ref, ref, dev(c=1 - c), "od", kind).wait_send()

    events = {}

    def event(name):
        def add(f):
            events[name] = f
        return add

    halo_r = describe(X.at[pl.ds(128, 16)], X.at[pl.ds(0, 16)], {"sp": nxt, "dp": dp}, "hr", "hr")
    halo_l = describe(X.at[pl.ds(16, 16)], X.at[pl.ds(144, 16)], {"sp": prev, "dp": dp}, "hl", "hl")
    lo, hi = pl.ds(0, 2), pl.ds(2, 2)

    @event("halo")
    def _():
        @pl.when(sp < 63)
        def _():
            halo_r.start()

        @pl.when(sp > 0)
        def _():
            halo_l.start()

        T[...] = TB[...].astype(jnp.float32)

    @event("ox")
    def _():
        for d in (1, 3, 2):
            send("ox", O.at[x, c, z, y], dev(x=mod(x + d, 4)))

    @event("oy")
    def _():
        arrived("ox", O.at[pl.ds(0, 3), c, z, y])
        for d in (1, 3, 2):
            send("oy", O.at[:, c, z, y], dev(y=mod(y + d, 4)))

    stepped = [0] * 9

    def ring(s, h):
        zo, zp = mod(z - s, 16), mod(z + s, 16)
        if s > 0:
            arrived(("ring", s - 1, h), O.at[:, c, z, pl.ds(0, 2 if s < 8 else 1)])
        if s < 7 or (s == 7 and h < 2):
            send(("ring", s, h), O.at[:, c, zo, h], dev(z=zr))
        if s < 7 or (s == 7 and h >= 2):
            send(("ring", s, h), O.at[:, c, zp, h], dev(z=zl))
        stepped[s] += 1
        if stepped[s] == 4:
            send("od", O.at[:, c, zo], dev(c=1 - c))
            if 0 < s < 8:
                send("od", O.at[:, c, zp], dev(c=1 - c))

    @event("g0")
    def _():
        arrived("oy", O.at[:, c, z, pl.ds(0, 3)])
        for h in range(4):
            ring(0, h)

    for s in range(1, 9):
        for h in range(4):
            event(f"g{s}_{h}")(lambda s=s, h=h: ring(s, h))

    def s2(m):
        for p in peers:
            send(("s2", m), W.at[x, c, qs[m], r, y], dev(z=p))

    @event("s1")
    def _():
        s2(0)
        send("s1+", W.at[x, c, q, r, y], dev(z=z4r))
        send("s1-", W.at[x, c, q, r, y], dev(z=z4l))

    @event("s1l")
    def _():
        arrived("s1+", W.at[x, c, q, r, y])
        send("s1r", W.at[x, c, qs[1], r, y, 0], dev(z=z4r))
        s2(1)

    @event("s1r")
    def _():
        arrived("s1-", W.at[x, c, q, r, y])
        send("s1r", W.at[x, c, qs[2], r, y, 1], dev(z=z4l))
        s2(2)

    @event("s1rr")
    def _():
        arrived("s1r", W.at[x, c, q, r, y])
        s2(3)

    yn, xn = {"+": dev(y=yr), "-": dev(y=yl)}, {"+": dev(x=xr), "-": dev(x=xl)}
    at = {"o": 0, "+": -1, "-": 1, "x": 2}

    def part(T, m, p, rows=slice(None)):
        if T == "A":
            return W.at[x, c, qs[m], rows, mod(y + at[p], 4), 0]
        return W.at[mod(x + at[p], 4), c, qs[m], rows, y, 1]

    def slab(T, m, d, rows=slice(None)):
        if T == "A":
            return W.at[mod(x + at[d], 4), c, qs[m], rows, :, 0]
        return W.at[:, c, qs[m], rows, mod(y + at[d], 4), 1]

    ring1, ring2 = {"A": yn, "B": xn}, {"A": xn, "B": yn}
    half = {"+": lo, "-": hi}

    def p1(m):
        arrived(("s2", m), W.at[x, c, qs[m], pl.ds(0, 3), y])
        for T in "AB":
            for d in "+-":
                send(("p1", T, m, d), part(T, m, "o"), ring1[T][d])
            for d in "+-":
                send(("p2", T, m, d), part(T, m, "o"), ring2[T][d])
            if m in DIRECT:
                send(("p1r", T, m), part(T, m, "o"), dev(y=mod(y + 2, 4)) if T == "A" else dev(x=mod(x + 2, 4)))

    def p1r(T, m, d):
        arrived(("p1", T, m, d), part(T, m, "o"))
        if m not in DIRECT:
            send(("p1r", T, m), part(T, m, d, half[d]), ring1[T][d])
        for e in "+-":
            send(("p2", T, m, e), part(T, m, d), ring2[T][e])

    def p2(T, m):
        arrived(("p1r", T, m), part(T, m, "o"))
        for e in "+-":
            send(("p2", T, m, e), part(T, m, "x"), ring2[T][e])
        send(("d2d", m), slab(T, m, "o"), dev(c=1 - c))

    def p2r(T, m, d):
        arrived(("p2", T, m, d), slab(T, m, d))
        send(("p2r", T, m), slab(T, m, d, half[d]), ring2[T][d])
        send(("d2d", m), slab(T, m, d), dev(c=1 - c))

    def d2d(T, m):
        arrived(("p2r", T, m), slab(T, m, "+"))
        send(("d2d", m), slab(T, m, "x"), dev(c=1 - c))

    def compute(m):
        arrived(("d2d", m), W.at[:, 1 - c, qs[m]])
        if m == FIRST:
            @pl.when(sp > 0)
            def _():
                halo_r.wait_recv()

            @pl.when(sp < 63)
            def _():
                halo_l.wait_recv()

        qm = qs[m]
        acc = [None, None]
        for i in range(8):
            xs = X[:, 256 * i : 256 * i + 256]
            for k in (0, 1):
                w = W[i // 2, i % 2, qm, :, :, k].reshape(256, 256)
                part = lax.dot_general(xs, w, NT, preferred_element_type=jnp.float32)
                acc[k] = part if acc[k] is None else acc[k] + part
        gated = (acc[0] * jax.nn.sigmoid(acc[1])).astype(jnp.bfloat16).astype(jnp.float32)
        for h in (0, 1):
            strip = gated[:, 128 * h : 128 * h + 128]
            lanes = pl.ds(pl.multiple_of(qm * 256 + 128 * h, 128), 128)
            total = jnp.zeros((128, 128), jnp.float32)
            for shift in range(8):
                rolled = strip if shift == 0 else pltpu.roll(strip, 160 - shift, 0)
                for k in range(31):
                    if (k + 1) % 8 == shift:
                        first = (k + 1) // 8 * 8
                        total = total + T[pl.ds(k, 1), lanes] * rolled[first : first + 128]
            CV[:, lanes] = total.astype(jnp.bfloat16).astype(jnp.float32)

    for m in range(4):
        event(f"p1_{m}")(lambda m=m: p1(m))
        event(f"c_{m}")(lambda m=m: compute(m))
        for T_ in "AB":
            event(f"p2{T_}_{m}")(lambda m=m, T_=T_: p2(T_, m))
            event(f"d{T_}_{m}")(lambda m=m, T_=T_: d2d(T_, m))
            for d in "+-":
                event(f"p1r{T_}{m}{d}")(lambda m=m, T_=T_, d=d: p1r(T_, m, d))
                event(f"p2r{T_}{m}{d}")(lambda m=m, T_=T_, d=d: p2r(T_, m, d))

    for name in ORDER:
        with jax.named_scope(name):
            events[name]()

    assert len(groups) == NSEM and len(kinds) == 13, (len(groups), len(kinds))

    def norm(i, carry):
        rows = pl.ds(pl.multiple_of(i * 16, 16), 16)
        v = CV[rows, :]
        mean = jnp.mean(v, axis=-1, keepdims=True)
        cen = v - mean
        var = jnp.mean(cen * cen, axis=-1, keepdims=True)
        n = cen * lax.rsqrt(var + 1e-05) * gain[...] + bias[...]
        ACT[rows, :] = (n * jax.nn.sigmoid(n)).astype(jnp.bfloat16)
        return carry

    with jax.named_scope("norm"):
        lax.fori_loop(0, 8, norm, 0, unroll=4)

    with jax.named_scope("out_rows"):
        arrived("od", O.at[:, 1 - c])

    def project(j, carry):
        acc = None
        zs = pl.ds(j * 4, 4)
        for i in range(4):
            w = jnp.concatenate([O[i, 0, zs].reshape(512, 128), O[i, 1, zs].reshape(512, 128)], axis=1)
            part = lax.dot_general(
                ACT[:, 256 * i : 256 * i + 256], w, NT, preferred_element_type=jnp.float32
            )
            acc = part if acc is None else acc + part
        out[:, pl.ds(pl.multiple_of(j * 512, 512), 512)] = acc.astype(jnp.bfloat16)
        return carry

    with jax.named_scope("project"):
        lax.fori_loop(0, 4, project, 0)

    with jax.named_scope("drain"):
        sent("p2", W.at[pl.ds(0, 2), c])
        sent("p2r", W.at[0, c])
        sent("p1", W.at[0, c, pl.ds(0, 2)])
        sent("p1r", W.at[0, c, 0])
        sent("d2d", W.at[:, c])
        sent("s2", W.at[0, c, 0, pl.ds(0, 3)])
        sent("s1", W.at[0, c, 0, pl.ds(0, 3), 0])
        sent("ox", O.at[0, c, 0, pl.ds(0, 3)])
        sent("oy", O.at[pl.ds(0, 3), c, 0])
        sent("ring", O.at[:, c, pl.ds(0, 15)])
        sent("od", O.at[:, c])

    @pl.when(sp < 63)
    def _():
        halo_r.wait_send()

    @pl.when(sp > 0)
    def _():
        halo_l.wait_send()


def on_device(tokens, w_value, w_gate, w_out, conv_taps, norm_gain, norm_bias):
    hbm = pl.BlockSpec(memory_space=pltpu.HBM)
    vmem = pl.BlockSpec(memory_space=pltpu.VMEM)
    mixed = pl.pallas_call(
        kernel,
        out_shape=jax.ShapeDtypeStruct((128, 2048), jnp.bfloat16),
        in_specs=[hbm] * 7,
        out_specs=vmem,
        scratch_shapes=[
            pltpu.VMEM((4, 2, 4, 4, 4, 2, 16, 256), jnp.bfloat16),
            pltpu.VMEM((4, 2, 16, 4, 32, 128), jnp.bfloat16),
            pltpu.VMEM((160, 2048), jnp.bfloat16),
            pltpu.VMEM((31, 1024), jnp.bfloat16),
            pltpu.VMEM((31, 1024), jnp.float32),
            pltpu.VMEM((1, 1024), jnp.float32),
            pltpu.VMEM((1, 1024), jnp.float32),
            pltpu.VMEM((128, 1024), jnp.float32),
            pltpu.VMEM((128, 1024), jnp.bfloat16),
            pltpu.SemaphoreType.DMA((13,)),
            pltpu.SemaphoreType.DMA((NSEM,)),
            pltpu.SemaphoreType.DMA((7,)),
        ],
        compiler_params=pltpu.CompilerParams(
            collective_id=0, has_side_effects=True, vmem_limit_bytes=50000000
        ),
    )(
        *[
            pltpu.with_memory_space_constraint(a, pltpu.HBM)
            for a in (
                tokens[0], w_value.T, w_gate.T, w_out.T, conv_taps.T, norm_gain[None, :], norm_bias[None, :],
            )
        ]
    )
    return mixed[None]


def solution(mesh):
    in_specs = (P("dp", "sp", None), P("dp", "sp"), P("dp", "sp"), P("dp", "sp"), P(), P(), P())
    out_specs = P("dp", "sp", None)
    return jax.shard_map(
        on_device, mesh=mesh, in_specs=in_specs, out_specs=out_specs, check_vma=False
    )
```

```python
import jax
import jax.numpy as jnp
from jax import lax
from jax.experimental import pallas as pl
from jax.experimental.pallas import tpu as pltpu
from jax.sharding import PartitionSpec as P

MESH = pl.DeviceIdType.MESH
NSEM = 96
ORDER = [
    "s1", "ox", "halo", "oy", "p1_0", "s1l", "s1r", "p1rA0-", "g0", "p1rA0+", "s1rr", "p1rB0+", "p2A_0",
    "p1rB0-", "p2B_0", "p1_1", "g1_0", "g1_1", "p1_2", "g1_3", "g1_2", "p2rA0-", "p2rA0+", "p1rB1+", "g2_0",
    "p2rB0-", "p1rA1+", "p1rA1-", "g2_1", "p1_3", "p1rB2+", "p1rB1-", "g2_3", "g2_2", "p1rA2-", "p1rA2+",
    "p1rB2-", "g3_0", "p2rB0+", "g3_1", "g3_3", "p1rA3+", "p2A_1", "g3_2", "dA_0", "p2B_1", "p1rA3-", "g4_0",
    "g4_1", "p1rB3+", "p1rB3-", "g4_3", "g4_2", "p2A_2", "p2B_2", "g5_0", "p2rA1+", "p2rA1-", "g5_1",
    "p2rB1+", "p2A_3", "p2rB1-", "dB_0", "p2B_3", "g5_3", "g5_2", "g6_0", "p2rB2+", "p2rB2-", "p2rA2-",
    "g6_1", "dA_1", "dB_1", "p2rA2+", "p2rA3+", "p2rA3-", "g6_3", "p2rB3+", "g6_2", "p2rB3-", "c_0", "g7_0",
    "g7_1", "dB_2", "dA_2", "g7_3", "g7_2", "dA_3", "dB_3", "c_1", "c_2", "g8_1", "g8_3", "g8_0", "g8_2",
    "c_3",
]
SENDS = {"ox": "ox", "oy": "oy",
         "s1+": "s1", "s1-": "s1", "s1r": "s1", "od": "od"}
FIRST = 0
DIRECT = (0,)
NT = (((1,), (1,)), ((), ()))


def kernel(
    tok, wv, wg, wo, taps_in, gain_in, bias_in, out,
    W, O, X, TB, T, gain, bias, CV, ACT, ssem, rsem, lsem,
):
    sp = lax.axis_index("sp")
    dp = lax.axis_index("dp")
    z, y = sp // 4, lax.rem(sp, 4)
    x, c = dp // 2, lax.rem(dp, 2)
    q, r = z // 4, lax.rem(z, 4)

    def dev(x=x, y=y, z=z, c=c):
        return {"sp": z * 4 + y, "dp": x * 2 + c}

    def mod(v, n):
        return lax.rem(v + n, n)

    xl, xr = mod(x - 1, 4), mod(x + 1, 4)
    yl, yr = mod(y - 1, 4), mod(y + 1, 4)
    zl, zr = mod(z - 1, 16), mod(z + 1, 16)
    z4l, z4r = mod(z - 4, 16), mod(z + 4, 16)
    peers = [q * 4 + mod(r + d, 4) for d in (1, 2, 3)]
    qs = [q, mod(q - 1, 4), mod(q + 1, 4), mod(q + 2, 4)]
    prev, nxt = mod(sp - 1, 64), mod(sp + 1, 64)

    local = [
        pltpu.make_async_copy(wv, W.at[x, c, q, r, y, 0], lsem.at[0]),
        pltpu.make_async_copy(wg, W.at[x, c, q, r, y, 1], lsem.at[1]),
        pltpu.make_async_copy(wo, O.at[x, c, z, y], lsem.at[2]),
        pltpu.make_async_copy(tok, X.at[pl.ds(16, 128)], lsem.at[3]),
        pltpu.make_async_copy(taps_in, TB, lsem.at[4]),
        pltpu.make_async_copy(gain_in, gain, lsem.at[5]),
        pltpu.make_async_copy(bias_in, bias, lsem.at[6]),
    ]
    for d in local:
        d.start()

    barrier = pltpu.get_barrier_semaphore()
    partners = [dev(x=xl), dev(x=xr), dev(y=yl), dev(y=yr), dev(z=zl), dev(z=zr), dev(z=z4l), dev(z=z4r)]
    partners += [dev(z=p) for p in peers]
    partners += [dev(x=mod(x + 2, 4)), dev(y=mod(y + 2, 4))]
    partners += [dev(c=1 - c), {"sp": prev, "dp": dp}, {"sp": nxt, "dp": dp}]
    for p in partners:
        pl.semaphore_signal(barrier, inc=1, device_id=p, device_id_type=MESH)

    @pl.when(sp == 0)
    def _():
        X[pl.ds(0, 16), :] = jnp.zeros((16, 2048), jnp.bfloat16)

    @pl.when(sp == 63)
    def _():
        X[pl.ds(144, 16), :] = jnp.zeros((16, 2048), jnp.bfloat16)

    with jax.named_scope("barrier"):
        for d in local:
            d.wait()
        pl.semaphore_wait(barrier, len(partners))

    groups = {}

    kinds = {}

    def describe(src, dst, to, key, kind):
        i = groups.setdefault(key, len(groups))
        j = kinds.setdefault(kind, len(kinds))
        return pltpu.make_async_remote_copy(
            src_ref=src, dst_ref=dst, send_sem=ssem.at[j], recv_sem=rsem.at[i],
            device_id=to, device_id_type=MESH,
        )

    def send(key, ref, to):
        kind = key[0] if isinstance(key, tuple) else SENDS[key]
        describe(ref, ref, to, key, kind).start()

    def arrived(key, ref):
        describe(ref, ref, dev(c=1 - c), key, "d2d").wait_recv()

    def sent(kind, ref):
        describe(ref, ref, dev(c=1 - c), "od", kind).wait_send()

    events = {}

    def event(name):
        def add(f):
            events[name] = f
        return add

    halo_r = describe(X.at[pl.ds(128, 16)], X.at[pl.ds(0, 16)], {"sp": nxt, "dp": dp}, "hr", "hr")
    halo_l = describe(X.at[pl.ds(16, 16)], X.at[pl.ds(144, 16)], {"sp": prev, "dp": dp}, "hl", "hl")
    lo, hi = pl.ds(0, 2), pl.ds(2, 2)

    @event("halo")
    def _():
        @pl.when(sp < 63)
        def _():
            halo_r.start()

        @pl.when(sp > 0)
        def _():
            halo_l.start()

        T[...] = TB[...].astype(jnp.float32)

    @event("ox")
    def _():
        for d in (1, 3, 2):
            send("ox", O.at[x, c, z, y], dev(x=mod(x + d, 4)))

    @event("oy")
    def _():
        arrived("ox", O.at[pl.ds(0, 3), c, z, y])
        for d in (1, 3, 2):
            send("oy", O.at[:, c, z, y], dev(y=mod(y + d, 4)))

    stepped = [0] * 9

    def ring(s, h):
        zo, zp = mod(z - s, 16), mod(z + s, 16)
        if s > 0:
            arrived(("ring", s - 1, h), O.at[:, c, z, pl.ds(0, 2 if s < 8 else 1)])
        if s < 7 or (s == 7 and h < 2):
            send(("ring", s, h), O.at[:, c, zo, h], dev(z=zr))
        if s < 7 or (s == 7 and h >= 2):
            send(("ring", s, h), O.at[:, c, zp, h], dev(z=zl))
        stepped[s] += 1
        if stepped[s] == 4:
            send("od", O.at[:, c, zo], dev(c=1 - c))
            if 0 < s < 8:
                send("od", O.at[:, c, zp], dev(c=1 - c))

    @event("g0")
    def _():
        arrived("oy", O.at[:, c, z, pl.ds(0, 3)])
        for h in range(4):
            ring(0, h)

    for s in range(1, 9):
        for h in range(4):
            event(f"g{s}_{h}")(lambda s=s, h=h: ring(s, h))

    def s2(m):
        for p in peers:
            send(("s2", m), W.at[x, c, qs[m], r, y], dev(z=p))

    @event("s1")
    def _():
        s2(0)
        send("s1+", W.at[x, c, q, r, y], dev(z=z4r))
        send("s1-", W.at[x, c, q, r, y], dev(z=z4l))

    @event("s1l")
    def _():
        arrived("s1+", W.at[x, c, q, r, y])
        send("s1r", W.at[x, c, qs[1], r, y, 0], dev(z=z4r))
        s2(1)

    @event("s1r")
    def _():
        arrived("s1-", W.at[x, c, q, r, y])
        send("s1r", W.at[x, c, qs[2], r, y, 1], dev(z=z4l))
        s2(2)

    @event("s1rr")
    def _():
        arrived("s1r", W.at[x, c, q, r, y])
        s2(3)

    yn, xn = {"+": dev(y=yr), "-": dev(y=yl)}, {"+": dev(x=xr), "-": dev(x=xl)}
    at = {"o": 0, "+": -1, "-": 1, "x": 2}

    def part(T, m, p, rows=slice(None)):
        if T == "A":
            return W.at[x, c, qs[m], rows, mod(y + at[p], 4), 0]
        return W.at[mod(x + at[p], 4), c, qs[m], rows, y, 1]

    def slab(T, m, d, rows=slice(None)):
        if T == "A":
            return W.at[mod(x + at[d], 4), c, qs[m], rows, :, 0]
        return W.at[:, c, qs[m], rows, mod(y + at[d], 4), 1]

    ring1, ring2 = {"A": yn, "B": xn}, {"A": xn, "B": yn}
    half = {"+": lo, "-": hi}

    def p1(m):
        arrived(("s2", m), W.at[x, c, qs[m], pl.ds(0, 3), y])
        for T in "AB":
            for d in "+-":
                send(("p1", T, m, d), part(T, m, "o"), ring1[T][d])
            for d in "+-":
                send(("p2", T, m, d), part(T, m, "o"), ring2[T][d])
            if m in DIRECT:
                send(("p1r", T, m), part(T, m, "o"), dev(y=mod(y + 2, 4)) if T == "A" else dev(x=mod(x + 2, 4)))

    def p1r(T, m, d):
        arrived(("p1", T, m, d), part(T, m, "o"))
        if m not in DIRECT:
            send(("p1r", T, m), part(T, m, d, half[d]), ring1[T][d])
        for e in "+-":
            send(("p2", T, m, e), part(T, m, d), ring2[T][e])

    def p2(T, m):
        arrived(("p1r", T, m), part(T, m, "o"))
        for e in "+-":
            send(("p2", T, m, e), part(T, m, "x"), ring2[T][e])
        send(("d2d", m), slab(T, m, "o"), dev(c=1 - c))

    def p2r(T, m, d):
        arrived(("p2", T, m, d), slab(T, m, d))
        send(("p2r", T, m), slab(T, m, d, half[d]), ring2[T][d])
        send(("d2d", m), slab(T, m, d), dev(c=1 - c))

    def d2d(T, m):
        arrived(("p2r", T, m), slab(T, m, "+"))
        send(("d2d", m), slab(T, m, "x"), dev(c=1 - c))

    def compute(m):
        arrived(("d2d", m), W.at[:, 1 - c, qs[m]])
        if m == FIRST:
            @pl.when(sp > 0)
            def _():
                halo_r.wait_recv()

            @pl.when(sp < 63)
            def _():
                halo_l.wait_recv()

        qm = qs[m]
        acc = [None, None]
        for i in range(8):
            xs = X[:, 256 * i : 256 * i + 256]
            for k in (0, 1):
                w = W[i // 2, i % 2, qm, :, :, k].reshape(256, 256)
                part = lax.dot_general(xs, w, NT, preferred_element_type=jnp.float32)
                acc[k] = part if acc[k] is None else acc[k] + part
        gated = (acc[0] * jax.nn.sigmoid(acc[1])).astype(jnp.bfloat16).astype(jnp.float32)
        for h in (0, 1):
            strip = gated[:, 128 * h : 128 * h + 128]
            lanes = pl.ds(pl.multiple_of(qm * 256 + 128 * h, 128), 128)
            total = jnp.zeros((128, 128), jnp.float32)
            for shift in range(8):
                rolled = strip if shift == 0 else pltpu.roll(strip, 160 - shift, 0)
                for k in range(31):
                    if (k + 1) % 8 == shift:
                        first = (k + 1) // 8 * 8
                        total = total + T[pl.ds(k, 1), lanes] * rolled[first : first + 128]
            CV[:, lanes] = total.astype(jnp.bfloat16).astype(jnp.float32)

    for m in range(4):
        event(f"p1_{m}")(lambda m=m: p1(m))
        event(f"c_{m}")(lambda m=m: compute(m))
        for T_ in "AB":
            event(f"p2{T_}_{m}")(lambda m=m, T_=T_: p2(T_, m))
            event(f"d{T_}_{m}")(lambda m=m, T_=T_: d2d(T_, m))
            for d in "+-":
                event(f"p1r{T_}{m}{d}")(lambda m=m, T_=T_, d=d: p1r(T_, m, d))
                event(f"p2r{T_}{m}{d}")(lambda m=m, T_=T_, d=d: p2r(T_, m, d))

    for name in ORDER:
        with jax.named_scope(name):
            events[name]()

    assert len(groups) == NSEM and len(kinds) == 13, (len(groups), len(kinds))

    def norm(i, carry):
        rows = pl.ds(pl.multiple_of(i * 16, 16), 16)
        v = CV[rows, :]
        mean = jnp.mean(v, axis=-1, keepdims=True)
        cen = v - mean
        var = jnp.mean(cen * cen, axis=-1, keepdims=True)
        n = cen * lax.rsqrt(var + 1e-05) * gain[...] + bias[...]
        ACT[rows, :] = (n * jax.nn.sigmoid(n)).astype(jnp.bfloat16)
        return carry

    with jax.named_scope("norm"):
        lax.fori_loop(0, 8, norm, 0, unroll=8)

    with jax.named_scope("out_rows"):
        arrived("od", O.at[:, 1 - c])

    def project(j, carry):
        acc = None
        zs = pl.ds(j * 4, 4)
        for i in range(4):
            w = jnp.concatenate([O[i, 0, zs].reshape(512, 128), O[i, 1, zs].reshape(512, 128)], axis=1)
            part = lax.dot_general(
                ACT[:, 256 * i : 256 * i + 256], w, NT, preferred_element_type=jnp.float32
            )
            acc = part if acc is None else acc + part
        out[:, pl.ds(pl.multiple_of(j * 512, 512), 512)] = acc.astype(jnp.bfloat16)
        return carry

    with jax.named_scope("project"):
        lax.fori_loop(0, 4, project, 0, unroll=4)

    with jax.named_scope("drain"):
        sent("p2", W.at[pl.ds(0, 2), c])
        sent("p2r", W.at[0, c])
        sent("p1", W.at[0, c, pl.ds(0, 2)])
        sent("p1r", W.at[0, c, 0])
        sent("d2d", W.at[:, c])
        sent("s2", W.at[0, c, 0, pl.ds(0, 3)])
        sent("s1", W.at[0, c, 0, pl.ds(0, 3), 0])
        sent("ox", O.at[0, c, 0, pl.ds(0, 3)])
        sent("oy", O.at[pl.ds(0, 3), c, 0])
        sent("ring", O.at[:, c, pl.ds(0, 15)])
        sent("od", O.at[:, c])

    @pl.when(sp < 63)
    def _():
        halo_r.wait_send()

    @pl.when(sp > 0)
    def _():
        halo_l.wait_send()


def on_device(tokens, w_value, w_gate, w_out, conv_taps, norm_gain, norm_bias):
    hbm = pl.BlockSpec(memory_space=pltpu.HBM)
    vmem = pl.BlockSpec(memory_space=pltpu.VMEM)
    mixed = pl.pallas_call(
        kernel,
        out_shape=jax.ShapeDtypeStruct((128, 2048), jnp.bfloat16),
        in_specs=[hbm] * 7,
        out_specs=vmem,
        scratch_shapes=[
            pltpu.VMEM((4, 2, 4, 4, 4, 2, 16, 256), jnp.bfloat16),
            pltpu.VMEM((4, 2, 16, 4, 32, 128), jnp.bfloat16),
            pltpu.VMEM((160, 2048), jnp.bfloat16),
            pltpu.VMEM((31, 1024), jnp.bfloat16),
            pltpu.VMEM((31, 1024), jnp.float32),
            pltpu.VMEM((1, 1024), jnp.float32),
            pltpu.VMEM((1, 1024), jnp.float32),
            pltpu.VMEM((128, 1024), jnp.float32),
            pltpu.VMEM((128, 1024), jnp.bfloat16),
            pltpu.SemaphoreType.DMA((13,)),
            pltpu.SemaphoreType.DMA((NSEM,)),
            pltpu.SemaphoreType.DMA((7,)),
        ],
        compiler_params=pltpu.CompilerParams(
            collective_id=0, has_side_effects=True, vmem_limit_bytes=50000000
        ),
    )(
        *[
            pltpu.with_memory_space_constraint(a, pltpu.HBM)
            for a in (
                tokens[0], w_value.T, w_gate.T, w_out.T, conv_taps.T, norm_gain[None, :], norm_bias[None, :],
            )
        ]
    )
    return mixed[None]


def solution(mesh):
    in_specs = (P("dp", "sp", None), P("dp", "sp"), P("dp", "sp"), P("dp", "sp"), P(), P(), P())
    out_specs = P("dp", "sp", None)
    return jax.shard_map(
        on_device, mesh=mesh, in_specs=in_specs, out_specs=out_specs, check_vma=False
    )
```

```python
import jax
import jax.numpy as jnp
from jax import lax
from jax.experimental import pallas as pl
from jax.experimental.pallas import tpu as pltpu
from jax.sharding import PartitionSpec as P

MESH = pl.DeviceIdType.MESH
NSEM = 96
ORDER = [
    "s1", "ox", "halo", "oy", "p1_0", "s1l", "s1r", "p1rA0-", "g0", "p1rA0+", "s1rr", "p1rB0+", "p2A_0",
    "p1rB0-", "p2B_0", "p1_1", "g1_0", "g1_1", "p1_2", "g1_3", "g1_2", "p2rA0-", "p2rA0+", "p1rB1+", "g2_0",
    "p2rB0-", "p1rA1+", "p1rA1-", "g2_1", "p1_3", "p1rB2+", "p1rB1-", "g2_3", "g2_2", "p1rA2-", "p1rA2+",
    "p1rB2-", "g3_0", "p2rB0+", "g3_1", "g3_3", "p1rA3+", "p2A_1", "g3_2", "dA_0", "p2B_1", "p1rA3-", "g4_0",
    "g4_1", "p1rB3+", "p1rB3-", "g4_3", "g4_2", "p2A_2", "p2B_2", "g5_0", "p2rA1+", "p2rA1-", "g5_1",
    "p2rB1+", "p2A_3", "p2rB1-", "dB_0", "p2B_3", "g5_3", "g5_2", "g6_0", "p2rB2+", "p2rB2-", "p2rA2-",
    "g6_1", "dA_1", "dB_1", "p2rA2+", "p2rA3+", "p2rA3-", "g6_3", "p2rB3+", "g6_2", "p2rB3-", "c_0", "g7_0",
    "g7_1", "dB_2", "dA_2", "g7_3", "g7_2", "dA_3", "dB_3", "c_1", "g8_1", "g8_3", "g8_0", "g8_2", "c_2",
    "c_3",
]
SENDS = {"ox": "ox", "oy": "oy",
         "s1+": "s1", "s1-": "s1", "s1r": "s1", "od": "od"}
FIRST = 0
DIRECT = (0,)
NT = (((1,), (1,)), ((), ()))


def kernel(
    tok, wv, wg, wo, taps_in, gain_in, bias_in, out,
    W, O, X, TB, T, gain, bias, CV, ACT, ssem, rsem, lsem,
):
    sp = lax.axis_index("sp")
    dp = lax.axis_index("dp")
    z, y = sp // 4, lax.rem(sp, 4)
    x, c = dp // 2, lax.rem(dp, 2)
    q, r = z // 4, lax.rem(z, 4)

    def dev(x=x, y=y, z=z, c=c):
        return {"sp": z * 4 + y, "dp": x * 2 + c}

    def mod(v, n):
        return lax.rem(v + n, n)

    xl, xr = mod(x - 1, 4), mod(x + 1, 4)
    yl, yr = mod(y - 1, 4), mod(y + 1, 4)
    zl, zr = mod(z - 1, 16), mod(z + 1, 16)
    z4l, z4r = mod(z - 4, 16), mod(z + 4, 16)
    peers = [q * 4 + mod(r + d, 4) for d in (1, 2, 3)]
    qs = [q, mod(q - 1, 4), mod(q + 1, 4), mod(q + 2, 4)]
    prev, nxt = mod(sp - 1, 64), mod(sp + 1, 64)

    local = [
        pltpu.make_async_copy(wv, W.at[x, c, q, r, y, 0], lsem.at[0]),
        pltpu.make_async_copy(wg, W.at[x, c, q, r, y, 1], lsem.at[1]),
        pltpu.make_async_copy(wo, O.at[x, c, z, y], lsem.at[2]),
        pltpu.make_async_copy(tok, X.at[pl.ds(16, 128)], lsem.at[3]),
        pltpu.make_async_copy(taps_in, TB, lsem.at[4]),
        pltpu.make_async_copy(gain_in, gain, lsem.at[5]),
        pltpu.make_async_copy(bias_in, bias, lsem.at[6]),
    ]
    for d in local:
        d.start()

    barrier = pltpu.get_barrier_semaphore()
    partners = [dev(x=xl), dev(x=xr), dev(y=yl), dev(y=yr), dev(z=zl), dev(z=zr), dev(z=z4l), dev(z=z4r)]
    partners += [dev(z=p) for p in peers]
    partners += [dev(x=mod(x + 2, 4)), dev(y=mod(y + 2, 4))]
    partners += [dev(c=1 - c), {"sp": prev, "dp": dp}, {"sp": nxt, "dp": dp}]
    for p in partners:
        pl.semaphore_signal(barrier, inc=1, device_id=p, device_id_type=MESH)

    @pl.when(sp == 0)
    def _():
        X[pl.ds(0, 16), :] = jnp.zeros((16, 2048), jnp.bfloat16)

    @pl.when(sp == 63)
    def _():
        X[pl.ds(144, 16), :] = jnp.zeros((16, 2048), jnp.bfloat16)

    with jax.named_scope("barrier"):
        for d in local:
            d.wait()
        pl.semaphore_wait(barrier, len(partners))

    groups = {}

    kinds = {}

    def describe(src, dst, to, key, kind):
        i = groups.setdefault(key, len(groups))
        j = kinds.setdefault(kind, len(kinds))
        return pltpu.make_async_remote_copy(
            src_ref=src, dst_ref=dst, send_sem=ssem.at[j], recv_sem=rsem.at[i],
            device_id=to, device_id_type=MESH,
        )

    def send(key, ref, to):
        kind = key[0] if isinstance(key, tuple) else SENDS[key]
        describe(ref, ref, to, key, kind).start()

    def arrived(key, ref):
        describe(ref, ref, dev(c=1 - c), key, "d2d").wait_recv()

    def sent(kind, ref):
        describe(ref, ref, dev(c=1 - c), "od", kind).wait_send()

    events = {}

    def event(name):
        def add(f):
            events[name] = f
        return add

    halo_r = describe(X.at[pl.ds(128, 16)], X.at[pl.ds(0, 16)], {"sp": nxt, "dp": dp}, "hr", "hr")
    halo_l = describe(X.at[pl.ds(16, 16)], X.at[pl.ds(144, 16)], {"sp": prev, "dp": dp}, "hl", "hl")
    lo, hi = pl.ds(0, 2), pl.ds(2, 2)

    @event("halo")
    def _():
        @pl.when(sp < 63)
        def _():
            halo_r.start()

        @pl.when(sp > 0)
        def _():
            halo_l.start()

        T[...] = TB[...].astype(jnp.float32)

    @event("ox")
    def _():
        for d in (1, 3, 2):
            send("ox", O.at[x, c, z, y], dev(x=mod(x + d, 4)))

    @event("oy")
    def _():
        arrived("ox", O.at[pl.ds(0, 3), c, z, y])
        for d in (1, 3, 2):
            send("oy", O.at[:, c, z, y], dev(y=mod(y + d, 4)))

    stepped = [0] * 9

    def ring(s, h):
        zo, zp = mod(z - s, 16), mod(z + s, 16)
        if s > 0:
            arrived(("ring", s - 1, h), O.at[:, c, z, pl.ds(0, 2 if s < 8 else 1)])
        if s < 7 or (s == 7 and h < 2):
            send(("ring", s, h), O.at[:, c, zo, h], dev(z=zr))
        if s < 7 or (s == 7 and h >= 2):
            send(("ring", s, h), O.at[:, c, zp, h], dev(z=zl))
        stepped[s] += 1
        if stepped[s] == 4:
            send("od", O.at[:, c, zo], dev(c=1 - c))
            if 0 < s < 8:
                send("od", O.at[:, c, zp], dev(c=1 - c))

    @event("g0")
    def _():
        arrived("oy", O.at[:, c, z, pl.ds(0, 3)])
        for h in range(4):
            ring(0, h)

    for s in range(1, 9):
        for h in range(4):
            event(f"g{s}_{h}")(lambda s=s, h=h: ring(s, h))

    def s2(m):
        for p in peers:
            send(("s2", m), W.at[x, c, qs[m], r, y], dev(z=p))

    @event("s1")
    def _():
        s2(0)
        send("s1+", W.at[x, c, q, r, y], dev(z=z4r))
        send("s1-", W.at[x, c, q, r, y], dev(z=z4l))

    @event("s1l")
    def _():
        arrived("s1+", W.at[x, c, q, r, y])
        send("s1r", W.at[x, c, qs[1], r, y, 0], dev(z=z4r))
        s2(1)

    @event("s1r")
    def _():
        arrived("s1-", W.at[x, c, q, r, y])
        send("s1r", W.at[x, c, qs[2], r, y, 1], dev(z=z4l))
        s2(2)

    @event("s1rr")
    def _():
        arrived("s1r", W.at[x, c, q, r, y])
        s2(3)

    yn, xn = {"+": dev(y=yr), "-": dev(y=yl)}, {"+": dev(x=xr), "-": dev(x=xl)}
    at = {"o": 0, "+": -1, "-": 1, "x": 2}

    def part(T, m, p, rows=slice(None)):
        if T == "A":
            return W.at[x, c, qs[m], rows, mod(y + at[p], 4), 0]
        return W.at[mod(x + at[p], 4), c, qs[m], rows, y, 1]

    def slab(T, m, d, rows=slice(None)):
        if T == "A":
            return W.at[mod(x + at[d], 4), c, qs[m], rows, :, 0]
        return W.at[:, c, qs[m], rows, mod(y + at[d], 4), 1]

    ring1, ring2 = {"A": yn, "B": xn}, {"A": xn, "B": yn}
    half = {"+": lo, "-": hi}

    def p1(m):
        arrived(("s2", m), W.at[x, c, qs[m], pl.ds(0, 3), y])
        for T in "AB":
            for d in "+-":
                send(("p1", T, m, d), part(T, m, "o"), ring1[T][d])
            for d in "+-":
                send(("p2", T, m, d), part(T, m, "o"), ring2[T][d])
            if m in DIRECT:
                send(("p1r", T, m), part(T, m, "o"), dev(y=mod(y + 2, 4)) if T == "A" else dev(x=mod(x + 2, 4)))

    def p1r(T, m, d):
        arrived(("p1", T, m, d), part(T, m, "o"))
        if m not in DIRECT:
            send(("p1r", T, m), part(T, m, d, half[d]), ring1[T][d])
        for e in "+-":
            send(("p2", T, m, e), part(T, m, d), ring2[T][e])

    def p2(T, m):
        arrived(("p1r", T, m), part(T, m, "o"))
        for e in "+-":
            send(("p2", T, m, e), part(T, m, "x"), ring2[T][e])
        send(("d2d", m), slab(T, m, "o"), dev(c=1 - c))

    def p2r(T, m, d):
        arrived(("p2", T, m, d), slab(T, m, d))
        send(("p2r", T, m), slab(T, m, d, half[d]), ring2[T][d])
        send(("d2d", m), slab(T, m, d), dev(c=1 - c))

    def d2d(T, m):
        arrived(("p2r", T, m), slab(T, m, "+"))
        send(("d2d", m), slab(T, m, "x"), dev(c=1 - c))

    def compute(m):
        arrived(("d2d", m), W.at[:, 1 - c, qs[m]])
        if m == FIRST:
            @pl.when(sp > 0)
            def _():
                halo_r.wait_recv()

            @pl.when(sp < 63)
            def _():
                halo_l.wait_recv()

        qm = qs[m]
        acc = [None, None]
        for i in range(8):
            xs = X[:, 256 * i : 256 * i + 256]
            for k in (0, 1):
                w = W[i // 2, i % 2, qm, :, :, k].reshape(256, 256)
                part = lax.dot_general(xs, w, NT, preferred_element_type=jnp.float32)
                acc[k] = part if acc[k] is None else acc[k] + part
        gated = (acc[0] * jax.nn.sigmoid(acc[1])).astype(jnp.bfloat16).astype(jnp.float32)
        for h in (0, 1):
            strip = gated[:, 128 * h : 128 * h + 128]
            lanes = pl.ds(pl.multiple_of(qm * 256 + 128 * h, 128), 128)
            total = jnp.zeros((128, 128), jnp.float32)
            for shift in range(8):
                rolled = strip if shift == 0 else pltpu.roll(strip, 160 - shift, 0)
                for k in range(31):
                    if (k + 1) % 8 == shift:
                        first = (k + 1) // 8 * 8
                        total = total + T[pl.ds(k, 1), lanes] * rolled[first : first + 128]
            CV[:, lanes] = total.astype(jnp.bfloat16).astype(jnp.float32)

    for m in range(4):
        event(f"p1_{m}")(lambda m=m: p1(m))
        event(f"c_{m}")(lambda m=m: compute(m))
        for T_ in "AB":
            event(f"p2{T_}_{m}")(lambda m=m, T_=T_: p2(T_, m))
            event(f"d{T_}_{m}")(lambda m=m, T_=T_: d2d(T_, m))
            for d in "+-":
                event(f"p1r{T_}{m}{d}")(lambda m=m, T_=T_, d=d: p1r(T_, m, d))
                event(f"p2r{T_}{m}{d}")(lambda m=m, T_=T_, d=d: p2r(T_, m, d))

    for name in ORDER:
        with jax.named_scope(name):
            events[name]()

    assert len(groups) == NSEM and len(kinds) == 13, (len(groups), len(kinds))

    def norm(i, carry):
        rows = pl.ds(pl.multiple_of(i * 16, 16), 16)
        v = CV[rows, :]
        mean = jnp.mean(v, axis=-1, keepdims=True)
        cen = v - mean
        var = jnp.mean(cen * cen, axis=-1, keepdims=True)
        n = cen * lax.rsqrt(var + 1e-05) * gain[...] + bias[...]
        ACT[rows, :] = (n * jax.nn.sigmoid(n)).astype(jnp.bfloat16)
        return carry

    with jax.named_scope("norm"):
        lax.fori_loop(0, 8, norm, 0, unroll=8)

    with jax.named_scope("out_rows"):
        arrived("od", O.at[:, 1 - c])

    def project(j, carry):
        acc = None
        zs = pl.ds(j * 4, 4)
        for i in range(4):
            w = jnp.concatenate([O[i, 0, zs].reshape(512, 128), O[i, 1, zs].reshape(512, 128)], axis=1)
            part = lax.dot_general(
                ACT[:, 256 * i : 256 * i + 256], w, NT, preferred_element_type=jnp.float32
            )
            acc = part if acc is None else acc + part
        out[:, pl.ds(pl.multiple_of(j * 512, 512), 512)] = acc.astype(jnp.bfloat16)
        return carry

    with jax.named_scope("project"):
        lax.fori_loop(0, 4, project, 0, unroll=4)

    with jax.named_scope("drain"):
        sent("p2", W.at[pl.ds(0, 2), c])
        sent("p2r", W.at[0, c])
        sent("p1", W.at[0, c, pl.ds(0, 2)])
        sent("p1r", W.at[0, c, 0])
        sent("d2d", W.at[:, c])
        sent("s2", W.at[0, c, 0, pl.ds(0, 3)])
        sent("s1", W.at[0, c, 0, pl.ds(0, 3), 0])
        sent("ox", O.at[0, c, 0, pl.ds(0, 3)])
        sent("oy", O.at[pl.ds(0, 3), c, 0])
        sent("ring", O.at[:, c, pl.ds(0, 15)])
        sent("od", O.at[:, c])

    @pl.when(sp < 63)
    def _():
        halo_r.wait_send()

    @pl.when(sp > 0)
    def _():
        halo_l.wait_send()


def on_device(tokens, w_value, w_gate, w_out, conv_taps, norm_gain, norm_bias):
    hbm = pl.BlockSpec(memory_space=pltpu.HBM)
    vmem = pl.BlockSpec(memory_space=pltpu.VMEM)
    mixed = pl.pallas_call(
        kernel,
        out_shape=jax.ShapeDtypeStruct((128, 2048), jnp.bfloat16),
        in_specs=[hbm] * 7,
        out_specs=vmem,
        scratch_shapes=[
            pltpu.VMEM((4, 2, 4, 4, 4, 2, 16, 256), jnp.bfloat16),
            pltpu.VMEM((4, 2, 16, 4, 32, 128), jnp.bfloat16),
            pltpu.VMEM((160, 2048), jnp.bfloat16),
            pltpu.VMEM((31, 1024), jnp.bfloat16),
            pltpu.VMEM((31, 1024), jnp.float32),
            pltpu.VMEM((1, 1024), jnp.float32),
            pltpu.VMEM((1, 1024), jnp.float32),
            pltpu.VMEM((128, 1024), jnp.float32),
            pltpu.VMEM((128, 1024), jnp.bfloat16),
            pltpu.SemaphoreType.DMA((13,)),
            pltpu.SemaphoreType.DMA((NSEM,)),
            pltpu.SemaphoreType.DMA((7,)),
        ],
        compiler_params=pltpu.CompilerParams(
            collective_id=0, has_side_effects=True, vmem_limit_bytes=50000000
        ),
    )(
        *[
            pltpu.with_memory_space_constraint(a, pltpu.HBM)
            for a in (
                tokens[0], w_value.T, w_gate.T, w_out.T, conv_taps.T, norm_gain[None, :], norm_bias[None, :],
            )
        ]
    )
    return mixed[None]


def solution(mesh):
    in_specs = (P("dp", "sp", None), P("dp", "sp"), P("dp", "sp"), P("dp", "sp"), P(), P(), P())
    out_specs = P("dp", "sp", None)
    return jax.shard_map(
        on_device, mesh=mesh, in_specs=in_specs, out_specs=out_specs, check_vma=False
    )
```
